512 devices in a mesh: sp: 32 (over z, core), tp: 16 (over y, x).
Axes of the slice: x: 4, y: 4, z: 16, core: 2. Of those that a mesh axis runs over, the one named last changes fastest.
Arguments:
- queries: bfloat16 [8192, 2048], P('sp', 'tp'), may hold values from -6 to 6
- keys: bfloat16 [8192, 1024], P('sp', 'tp'), may hold values from -6 to 6
- values: bfloat16 [8192, 1024], P('sp', 'tp'), may hold values from -6 to 6
- sink_logit: float32 [32], P('tp'), may hold values from -1 to 6
- out_weight: bfloat16 [2048, 2048], P(None, 'tp'), may hold values from -0.125 to 0.125
- residual: bfloat16 [8192, 2048], P(('sp', 'tp')), may hold values from -1.796875 to 1.796875
- norm_gain: float32 [2048], replicated, may hold values from 0.1 to 1.9
- routes: int32 [8192, 2], P(('sp', 'tp')), may hold values from 0 to 31, all different within a row; in each aligned block of 16 rows (0 to 15, 16 to 31, ...) at most 2 rows name the same one
- route_weights: float32 [8192, 2], P(('sp', 'tp')), may hold values from 0.2 to 1
- gate_weight: bfloat16 [32, 2048, 5120], P('sp', None, 'tp'), may hold values from -0.125 to 0.125
- up_weight: bfloat16 [32, 2048, 5120], P('sp', None, 'tp'), may hold values from -0.125 to 0.125
- down_weight: bfloat16 [32, 5120, 2048], P('sp', 'tp'), may hold values from -0.078125 to 0.078125
Outputs:
- mixed: bfloat16 [8192, 2048], P(('sp', 'tp'))
The draws below stay inside these ranges and needn't reach their ends.
Inputs may be any that keep to these rules, and one draw needn't show every extreme that they name: `routes`: each row names two different experts. Among the rows of one device no expert is named more than 2 times, and in every draw some expert is named exactly 2 times by the rows of some device.
All inputs are finite; a program needn't handle non-finite values.
Results may differ from the reference program's by a relative error of at most 0.018.
Values may be sent and summed in bfloat16 or wider, within the bound.
A program may use at most 64 MiB of HBM per device.

```python
import math
import jax
import jax.numpy as jnp
import numpy as np
from jax import lax

D = 2048
FF = 5120
HEADS = 32
KV_HEADS = 16
HEAD = 64
WINDOW = 128
TOK_DEV = 16
TOKENS = 8192
EXPERTS = 32
CAP = 2
N_SP = 32
N_TP = 16


def draw_queries(key, part):
    own_key = jax.random.fold_in(key, 17)
    drawn = jnp.clip(jax.random.normal(own_key, (TOKENS, HEADS * HEAD), jnp.float32), -6.0, 6.0)
    return drawn.astype(jnp.bfloat16)


def draw_keys(key, part):
    own_key = jax.random.fold_in(key, 29)
    drawn = jnp.clip(jax.random.normal(own_key, (TOKENS, KV_HEADS * HEAD), jnp.float32), -6.0, 6.0)
    return drawn.astype(jnp.bfloat16)


def shard_levels(stream_key, dims, cuts, smallest, top_value):
    level = 1.0
    for position, shards_of in cuts:
        steps = jax.random.uniform(jax.random.fold_in(jax.random.fold_in(stream_key, 6), position), (shards_of,), jnp.float32, smallest / len(cuts), top_value / len(cuts))
        level = level * jnp.repeat(jnp.exp(steps), dims[position] // shards_of).reshape((-1,) + (1,) * (len(dims) - 1 - position))
    return level


def deal_out(rng, own, number, rows, amount, top, limit, lean):
    order = jax.random.permutation(rng, amount)
    packed, ordinary = portions_of(amount, rows * top, limit, lean, True), portions_of(amount, rows * top, limit, lean, False)
    places = jnp.arange(amount)

    def named(tallies, rotation):
        used = int((tallies > 0).sum())
        fixed = max(1, used // 4)
        moved = fixed + (places - fixed + rotation * (used - fixed)) % max(1, amount - fixed)
        return jnp.zeros((amount,), jnp.int32).at[order[jnp.where(places < fixed, places, moved)]].set(jnp.asarray(tallies, jnp.int32))

    tallies = jnp.where(number % 4 == 0, named(packed, number // 4), named(ordinary, number - number // 4 - 1))
    mixed = jax.random.permutation(jax.random.fold_in(own, 3), amount)
    donor, taker = mixed[0:amount // 2 * 2:2], mixed[1:amount // 2 * 2:2]
    slack = jnp.minimum(tallies[donor] - 1, limit - tallies[taker]) // 2
    slack = jnp.where((donor == order[0]) | (taker == order[0]) | (tallies[taker] == 0), 0, jnp.maximum(slack, 0))
    moved = jax.random.randint(jax.random.fold_in(own, 4), (amount // 2,), 0, 1 << 20) % (slack + 1)
    tallies = tallies.at[donor].add(-moved).at[taker].add(moved)
    members = jnp.searchsorted(jnp.cumsum(tallies), jnp.arange(rows * top), side="right").astype(jnp.int32)
    listing = members.reshape(top, rows).T
    listing = listing[jax.random.permutation(jax.random.fold_in(own, 1), rows)]
    rotation = jax.random.randint(jax.random.fold_in(own, 2), (rows, 1), 0, top)
    return jnp.take_along_axis(listing, (jnp.arange(top)[None, :] + rotation) % top, axis=1)


def portions_of(amount, total, most, lean, full):
    loads = [(1 << 20) // math.isqrt(rank ** lean) + 1 for rank in range(1, amount + 1)]
    largest = most if full else min(most, max(-(-total // amount), total * loads[0] // sum(loads)))
    least = 1 if total - largest >= amount - 1 else 0
    counts, surplus = [largest] + [least] * (amount - 1), total - largest - least * (amount - 1)
    while surplus > 0:
        movable = [i for i in range(1, amount) if counts[i] < largest] or [i for i in range(1, amount) if counts[i] < most]
        pool, remaining = sum([loads[i] for i in movable]), surplus
        for i in movable:
            more = min(most - counts[i], max(1, remaining * loads[i] // pool), surplus)
            counts[i] = counts[i] + more
            surplus = surplus - more
    return np.array(counts)


def scatter_about(stream_key, extent, width, bound, shards=(), held_as=jnp.bfloat16):
    array = width * jax.random.normal(stream_key, extent, jnp.float32)
    if shards:
        array = array * shard_levels(stream_key, extent, shards, -0.22, 0.18)
    return jnp.clip(array, -bound, bound).astype(held_as)


def setup_inputs(seed: int = 0) -> dict:
    key_of = jax.random.split(jax.random.key(seed), 13)
    queries = draw_queries(jax.random.fold_in(key_of[12], 71), 0)
    keys = draw_keys(jax.random.fold_in(key_of[12], 71), 0)
    values = scatter_about(key_of[2], (TOKENS, KV_HEADS * HEAD), 1.0, 6.0, ((0, 32), (1, 16)))
    sink_logit = jnp.clip(-1.0 + 7.0 * jax.random.uniform(key_of[3], (HEADS,), jnp.float32) ** shard_levels(key_of[3], (HEADS,), ((0, 16),), -0.2, 0.2), -1.0, 6.0)
    out_weight = scatter_about(key_of[4], (HEADS * HEAD, D), (HEADS * HEAD) ** -0.5, 0.125, ((1, 16),))
    residual = scatter_about(key_of[5], (TOKENS, D), 0.3, 1.796875, ((0, 512),))
    norm_gain = jnp.clip(1.0 + 0.18 * jax.random.normal(key_of[6], (D,), jnp.float32), 0.1, 1.9)
    routes_keys = jax.random.split(jax.random.fold_in(key_of[7], 1), TOKENS // TOK_DEV)
    routes_turns = jax.random.permutation(jax.random.fold_in(key_of[7], 3), TOKENS // TOK_DEV)
    routes = jax.vmap(lambda own, number: deal_out(jax.random.fold_in(key_of[7], 2), own, number, TOK_DEV, EXPERTS, 2, CAP, 1))(routes_keys, routes_turns).reshape((TOKENS, 2))
    route_weights = jnp.clip(0.2 + 0.8 * jax.random.uniform(key_of[8], (TOKENS, 2), jnp.float32) ** shard_levels(key_of[8], (TOKENS, 2), ((0, 512),), -0.2, 0.2), 0.2, 1.0)
    gate_weight = scatter_about(key_of[9], (EXPERTS, D, FF), D ** -0.5, 0.125, ((0, 32), (2, 16)))
    up_weight = scatter_about(key_of[10], (EXPERTS, D, FF), D ** -0.5, 0.125, ((0, 32), (2, 16)))
    down_weight = scatter_about(key_of[11], (EXPERTS, FF, D), FF ** -0.5, 0.078125, ((0, 32), (1, 16)))
    return {"queries": queries, "keys": keys, "values": values, "sink_logit": sink_logit, "out_weight": out_weight, "residual": residual, "norm_gain": norm_gain, "routes": routes, "route_weights": route_weights, "gate_weight": gate_weight, "up_weight": up_weight, "down_weight": down_weight}


EPS = 1e-06
NEGATIVE = -1e+30

def make_band(tensor):
    length = tensor.shape[0]
    blocks = length // WINDOW
    padded = jnp.pad(tensor, ((WINDOW, WINDOW), (0, 0)))
    pieces = [padded[offset * WINDOW:offset * WINDOW + length].reshape(blocks, WINDOW, -1) for offset in range(3)]
    return jnp.concatenate(pieces, axis=1)

def attend(queries, keys, values, sink_logit):
    tokens = queries.shape[0]
    blocks = tokens // WINDOW
    repeat = HEADS // KV_HEADS
    scale = HEAD ** (-0.5)
    near = jnp.abs(jnp.arange(WINDOW)[:, None] + WINDOW - jnp.arange(3 * WINDOW)[None, :]) <= WINDOW
    key_pos = (jnp.arange(blocks)[:, None] - 1) * WINDOW + jnp.arange(3 * WINDOW)[None, :]
    inside = (key_pos >= 0) & (key_pos < tokens)
    valid = near[None, None, :, :] & inside[:, None, None, :]
    query_groups = queries.reshape(tokens, KV_HEADS, repeat, HEAD).transpose(1, 0, 2, 3)
    key_groups = keys.reshape(tokens, KV_HEADS, HEAD).transpose(1, 0, 2)
    value_groups = values.reshape(tokens, KV_HEADS, HEAD).transpose(1, 0, 2)
    sink_groups = sink_logit.reshape(KV_HEADS, repeat)

    def one_group(inputs):
        query_rows, key_rows, value_rows, sinks = inputs
        query_blocks = query_rows.reshape(blocks, WINDOW, repeat, HEAD).astype(jnp.float32)
        key_band = make_band(key_rows).astype(jnp.float32)
        value_band = make_band(value_rows).astype(jnp.float32)
        scores = jnp.einsum('nqrd,nkd->nrqk', query_blocks, key_band) * scale
        sink = sinks.astype(jnp.float32)[None, :, None, None]
        masked = jnp.where(valid, scores, NEGATIVE)
        top = jnp.maximum(lax.optimization_barrier(jnp.max(masked, axis=-1, keepdims=True)), sink)
        probs = jnp.exp(masked - top)
        denom = lax.optimization_barrier(jnp.sum(probs, axis=-1, keepdims=True)) + jnp.exp(sink - top)
        weights = (probs / denom).astype(jnp.bfloat16)
        output = jnp.einsum('nrqk,nkd->nqrd', weights.astype(jnp.float32), value_band)
        return output.astype(jnp.bfloat16).reshape(tokens, repeat * HEAD)
    outputs = lax.map(one_group, (query_groups, key_groups, value_groups, sink_groups))
    return outputs.transpose(1, 0, 2).reshape(tokens, HEADS * HEAD)

def one_expert(inputs):
    rows, gate_matrix, up_matrix, down_matrix = inputs
    gate = jnp.dot(rows, gate_matrix, preferred_element_type=jnp.float32)
    upward = jnp.dot(rows, up_matrix, preferred_element_type=jnp.float32)
    hidden = (jax.nn.silu(gate) * upward).astype(jnp.bfloat16)
    block_width = FF // N_TP
    shares = jnp.einsum('rjf,jfd->jrd', hidden.reshape(-1, N_TP, block_width).astype(jnp.float32), down_matrix.reshape(N_TP, block_width, D).astype(jnp.float32))
    return lax.optimization_barrier(jnp.sum(shares.astype(jnp.bfloat16).astype(jnp.float32), axis=0)).astype(jnp.bfloat16)

def reference(queries, keys, values, sink_logit, out_weight, residual, norm_gain, routes, route_weights, gate_weight, up_weight, down_weight):
    attention = attend(queries, keys, values, sink_logit)
    projected = jnp.dot(attention, out_weight, preferred_element_type=jnp.float32).astype(jnp.bfloat16)
    hidden_state = residual.astype(jnp.float32) + projected.astype(jnp.float32)
    inverse = lax.rsqrt(lax.optimization_barrier(jnp.mean(hidden_state * hidden_state, axis=-1, keepdims=True)) + EPS)
    normed = (hidden_state * inverse * norm_gain).astype(jnp.bfloat16)
    devices = N_SP * N_TP
    expert_ids = routes.reshape(devices, 2 * TOK_DEV).astype(jnp.int32)
    onehot = (expert_ids[..., None] == jnp.arange(EXPERTS, dtype=jnp.int32)).astype(jnp.int32)
    earlier = jnp.cumsum(onehot, axis=1) - onehot
    rank = lax.optimization_barrier(jnp.sum(earlier * onehot, axis=-1))
    slots = (jnp.arange(devices, dtype=jnp.int32)[:, None] * CAP + rank).reshape(-1).astype(jnp.int32)
    flat_ids = expert_ids.reshape(-1)
    pair_rows = jnp.repeat(normed, 2, axis=0)
    buffer = jnp.zeros((EXPERTS, devices * CAP, D), jnp.bfloat16).at[flat_ids, slots].set(pair_rows)
    expert_out = lax.map(one_expert, (buffer, gate_weight, up_weight, down_weight))
    picked = expert_out[flat_ids, slots].reshape(TOKENS, 2, D).astype(jnp.float32)
    mixture = lax.optimization_barrier(jnp.sum(route_weights[..., None] * picked, axis=1))
    return (hidden_state + mixture).astype(jnp.bfloat16)
```

```python
import functools

import jax
import jax.numpy as jnp
from jax import lax
from jax.experimental import pallas as pl
from jax.experimental.pallas import tpu as pltpu
from jax.sharding import PartitionSpec as P

HEADS = 32
KV_HEADS = 16
HEAD = 64
WINDOW = 128


EPS = 1e-06
NEGATIVE = -1e30


def with_halo(block, sides, width):
    for axis, dim in sides:
        count = lax.axis_size(axis)
        forward = [(i, i + 1) for i in range(count - 1)]
        backward = [(target, source) for source, target in forward]
        low = lax.ppermute(
            lax.slice_in_dim(block, block.shape[dim] - width, None, axis=dim), axis, forward
        )
        high = lax.ppermute(lax.slice_in_dim(block, 0, width, axis=dim), axis, backward)
        block = jnp.concatenate([low, block, high], axis=dim)
    return block


def sent_to_all(value, axis):
    copies = jnp.broadcast_to(value, (lax.axis_size(axis), *value.shape))
    return lax.all_to_all(copies, axis, split_axis=0, concat_axis=0, tiled=True)


def laid_out(tiles, dim):
    tiles = jnp.moveaxis(tiles, 0, dim)
    lengths = tiles.shape
    return tiles.reshape(*lengths[:dim], lengths[dim] * lengths[dim + 1], *lengths[dim + 2 :])


def gather_directly(value, axis, dim):
    tiles = sent_to_all(value, axis)
    return laid_out(tiles, dim)


def cut_along(value, dim, size):
    lengths = value.shape
    tiles = value.reshape(*lengths[:dim], size, lengths[dim] // size, *lengths[dim + 1 :])
    return jnp.moveaxis(tiles, dim, 0)


def summed_on_arrival(value, axis, dim):
    tiles = cut_along(value, dim, lax.axis_size(axis))
    arrived = lax.all_to_all(tiles, axis, split_axis=0, concat_axis=0, tiled=True)
    return arrived.astype(jnp.float32).sum(axis=0)


def make_band(extended, length):
    blocks = length // WINDOW
    pieces = [
        lax.slice_in_dim(extended, offset * WINDOW, offset * WINDOW + length, axis=0).reshape(
            blocks, WINDOW, -1
        )
        for offset in range(3)
    ]
    return jnp.concatenate(pieces, axis=1)


def attend_local(queries, keys, values, sink_logit):
    length = queries.shape[0]
    groups = keys.shape[1] // HEAD
    repeat = HEADS // KV_HEADS
    blocks = length // WINDOW
    joined = jnp.concatenate([keys, values], axis=1)
    extended = with_halo(joined, (("sp", 0),), WINDOW)
    banded = make_band(extended, length)
    key_band = banded[..., : groups * HEAD].reshape(blocks, 3 * WINDOW, groups, HEAD)
    value_band = banded[..., groups * HEAD :].reshape(blocks, 3 * WINDOW, groups, HEAD)
    query_blocks = queries.reshape(blocks, WINDOW, groups, repeat, HEAD)
    scores = jnp.einsum(
        "nqgrd,nkgd->ngrqk", query_blocks, key_band, preferred_element_type=jnp.float32
    ) * HEAD ** (-0.5)
    near = jnp.abs(jnp.arange(WINDOW)[:, None] + WINDOW - jnp.arange(3 * WINDOW)[None, :]) <= WINDOW
    first_token = lax.axis_index("sp") * length
    key_pos = (
        first_token + (jnp.arange(blocks)[:, None] - 1) * WINDOW + jnp.arange(3 * WINDOW)[None, :]
    )
    inside = (key_pos >= 0) & (key_pos < length * lax.axis_size("sp"))
    valid = near[None, None, None, :, :] & inside[:, None, None, None, :]
    sinks = sink_logit.reshape(1, groups, repeat, 1, 1)
    masked = jnp.where(valid, scores, NEGATIVE)
    top = jnp.maximum(jnp.max(masked, axis=-1, keepdims=True), sinks)
    probs = jnp.exp(masked - top)
    denom = jnp.sum(probs, axis=-1, keepdims=True) + jnp.exp(sinks - top)
    weights = (probs / denom).astype(jnp.bfloat16)
    output = jnp.einsum(
        "ngrqk,nkgd->nqgrd", weights, value_band, preferred_element_type=jnp.float32
    )
    return output.astype(jnp.bfloat16).reshape(length, groups * repeat * HEAD)


UNITS = 4
RING = 4
MESH = pl.DeviceIdType.MESH


def remote(src, dst, send_sem, recv_sem, device):
    return pltpu.make_async_remote_copy(
        src_ref=src, dst_ref=dst, send_sem=send_sem, recv_sem=recv_sem, device_id=device, device_id_type=MESH
    )


def moe_kernel(
    count,
    place_t_ref, first_ref, second_ref, rw_ref, normed_ref, hid_ref, wg_hbm, wu_hbm, wd_hbm,
    out_ref,
    wg, wu, wd, sending, arrived, x_all, p_all, half_s, full_s, sums, half_f, full_f, back_send, back,
    w_sem, d_send, d_recv, b_send, b_recv, g_send, g_recv,
):
    me = lax.axis_index("sp")
    tp = lax.axis_index("tp")
    ty, tx = tp // RING, lax.rem(tp, RING)
    rows = 2 * count // UNITS
    per = count // UNITS

    def shifted(pos, delta):
        return lax.rem(pos + (delta + RING), RING)

    def near(axis, delta):
        if axis == "x":
            return (me, ty * RING + shifted(tx, delta))
        return (me, shifted(ty, delta) * RING + tx)

    weight_copies = [
        pltpu.make_async_copy(wg_hbm.at[0], wg, w_sem.at[0]),
        pltpu.make_async_copy(wu_hbm.at[0], wu, w_sem.at[1]),
        pltpu.make_async_copy(wd_hbm.at[0], wd, w_sem.at[2]),
    ]
    for copy in weight_copies:
        copy.start()

    barrier = pltpu.get_barrier_semaphore()

    def greet(step, carry):
        pl.semaphore_signal(barrier, inc=1, device_id=(lax.rem(me + step, count), tp), device_id_type=MESH)
        return carry

    lax.fori_loop(1, count, greet, 0)
    for axis in ("x", "y"):
        for delta in (1, -1):
            pl.semaphore_signal(barrier, inc=1, device_id=near(axis, delta), device_id_type=MESH)

    slots = jnp.dot(place_t_ref[...], normed_ref[...], preferred_element_type=jnp.float32).astype(jnp.bfloat16)
    for expert in range(count):
        sending[expert] = slots[2 * expert : 2 * expert + 2, :]
    pl.semaphore_wait(barrier, count - 1 + 4)

    def dispatch(step):
        to = lax.rem(me + step, count)
        return remote(
            sending.at[to], arrived.at[count - step], d_send.at[step], d_recv.at[count - step], (to, tp)
        )

    def dispatch_pair(step, carry):
        dispatch(step).start()
        dispatch(count - step).start()
        return carry

    lax.fori_loop(1, count // 2, dispatch_pair, 0)
    dispatch(count // 2).start()
    arrived[0] = sending[me]

    axes = [("x", "y"), ("x", "y"), ("y", "x"), ("y", "x")]
    spot = {"x": tx, "y": ty}

    def gcopy(unit, number, src, dst, axis, delta):
        return remote(src, dst, g_send.at[unit, number], g_recv.at[unit, number], near(axis, delta))

    started = []

    def send(unit, number, src, dst, axis, delta):
        copy = gcopy(unit, number, src, dst, axis, delta)
        copy.start()
        started.append(copy)

    def landed(unit, number, dst):
        gcopy(unit, number, dst, dst, "x", 1).wait_recv()

    def g1(u):
        first, second = axes[u]
        f, s = spot[first], spot[second]
        pieces = []
        for j in range(per):
            o = u * per + j
            if o:
                remote(arrived.at[o], arrived.at[o], d_send.at[o], d_recv.at[o], (me, tp)).wait_recv()
            pieces.append(arrived[o])
        for j in range(per):
            x_all[u, s, f, 2 * j : 2 * j + 2, :] = pieces[j]
        own = x_all.at[u, s, f]
        send(u, 0, own, own, first, 1)
        send(u, 1, own, own, first, -1)

    def g2(u):
        first, second = axes[u]
        f, s = spot[first], spot[second]
        h = rows // 2
        low, high = x_all.at[u, s, shifted(f, -1)], x_all.at[u, s, shifted(f, 1)]
        landed(u, 0, low)
        send(u, 2, low.at[0:h], low.at[0:h], first, 1)
        landed(u, 1, high)
        send(u, 3, high.at[h:rows], high.at[h:rows], first, -1)

    def g3(u):
        first, second = axes[u]
        f, s = spot[first], spot[second]
        h = rows // 2
        far = x_all.at[u, s, shifted(f, 2)]
        landed(u, 2, far.at[0:h])
        landed(u, 3, far.at[h:rows])
        own = x_all.at[u, s]
        send(u, 4, own, own, second, 1)
        send(u, 5, own, own, second, -1)

    def g4(u):
        first, second = axes[u]
        s = spot[second]
        low, high = x_all.at[u, shifted(s, -1)], x_all.at[u, shifted(s, 1)]
        landed(u, 4, low)
        send(u, 6, low.at[0:2], low.at[0:2], second, 1)
        landed(u, 5, high)
        send(u, 7, high.at[2:4], high.at[2:4], second, -1)

    def mlp(u):
        first, second = axes[u]
        s = spot[second]
        far = x_all.at[u, shifted(s, 2)]
        landed(u, 6, far.at[0:2])
        landed(u, 7, far.at[2:4])
        width = x_all.shape[-1]
        flat = x_all[u].reshape(RING * RING * rows, width)
        gate = jnp.dot(flat, wg[...], preferred_element_type=jnp.float32)
        upward = jnp.dot(flat, wu[...], preferred_element_type=jnp.float32)
        hidden = (gate / (1.0 + jnp.exp(-gate)) * upward).astype(jnp.bfloat16)
        step = min(512, width)
        for n in range(0, width, step):
            part = jnp.dot(hidden, wd[:, n : n + step], preferred_element_type=jnp.float32)
            p_all[u, :, :, :, n : n + step] = part.astype(jnp.bfloat16).reshape(RING, RING, rows, step)

    def r1(u):
        first, second = axes[u]
        s = spot[second]
        far = p_all.at[u, shifted(s, 2)]
        send(u, 8, far.at[0:2], half_s.at[u, 0], second, 1)
        send(u, 9, far.at[2:4], half_s.at[u, 1], second, -1)

    def plus(a, b):
        return (a.astype(jnp.float32) + b.astype(jnp.float32)).astype(jnp.bfloat16)

    def r2(u):
        first, second = axes[u]
        s = spot[second]
        up, down = shifted(s, 1), shifted(s, -1)
        landed(u, 8, half_s.at[u, 0])
        p_all[u, up, 0:2] = plus(p_all[u, up, 0:2], half_s[u, 0])
        send(u, 10, p_all.at[u, up], full_s.at[u, 0], second, 1)
        landed(u, 9, half_s.at[u, 1])
        p_all[u, down, 2:4] = plus(p_all[u, down, 2:4], half_s[u, 1])
        send(u, 11, p_all.at[u, down], full_s.at[u, 1], second, -1)

    def r3(u):
        first, second = axes[u]
        f, s = spot[first], spot[second]
        h = rows // 2
        landed(u, 10, full_s.at[u, 0])
        landed(u, 11, full_s.at[u, 1])
        sums[u] = (
            p_all[u, s].astype(jnp.float32)
            + full_s[u, 0].astype(jnp.float32)
            + full_s[u, 1].astype(jnp.float32)
        ).astype(jnp.bfloat16)
        far = sums.at[u, shifted(f, 2)]
        send(u, 12, far.at[0:h], half_f.at[u, 0], first, 1)
        send(u, 13, far.at[h:rows], half_f.at[u, 1], first, -1)

    def r4(u):
        first, second = axes[u]
        f = spot[first]
        h = rows // 2
        up, down = shifted(f, 1), shifted(f, -1)
        landed(u, 12, half_f.at[u, 0])
        sums[u, up, 0:h] = plus(sums[u, up, 0:h], half_f[u, 0])
        send(u, 14, sums.at[u, up], full_f.at[u, 0], first, 1)
        landed(u, 13, half_f.at[u, 1])
        sums[u, down, h:rows] = plus(sums[u, down, h:rows], half_f[u, 1])
        send(u, 15, sums.at[u, down], full_f.at[u, 1], first, -1)

    def giving_back(o):
        to = lax.rem(me + o, count)
        return remote(back_send.at[o], back.at[me], b_send.at[o], b_recv.at[me], (to, tp))

    def r5(u):
        first, second = axes[u]
        f = spot[first]
        landed(u, 14, full_f.at[u, 0])
        landed(u, 15, full_f.at[u, 1])
        total = (
            sums[u, f].astype(jnp.float32)
            + full_f[u, 0].astype(jnp.float32)
            + full_f[u, 1].astype(jnp.float32)
        ).astype(jnp.bfloat16)
        for j in range(per):
            o = u * per + j
            if o:
                back_send[o] = total[2 * j : 2 * j + 2, :]
            else:
                back[me] = total[0:2, :]
        for j in range(per):
            o = u * per + j
            if o:
                giving_back(o).start()

    early, late = (0, 3), (1, 2)

    def run(stage, pair):
        for u in pair:
            stage(u)

    run(g1, early)
    run(g2, early)
    run(g1, late)
    run(g3, early)
    run(g2, late)
    run(g4, early)
    run(g3, late)
    for copy in weight_copies:
        copy.wait()
    for u in early:
        mlp(u)
        r1(u)
    run(g4, late)
    run(r2, early)
    for u in late:
        mlp(u)
        r1(u)
    run(r3, early)
    run(r2, late)
    run(r4, early)
    run(r3, late)
    run(r5, early)
    run(r4, late)
    run(r5, late)

    def came_back(step, carry):
        sender = lax.rem(me + step, count)
        remote(back.at[sender], back.at[sender], b_send.at[step], b_recv.at[sender], (me, tp)).wait_recv()
        return carry

    lax.fori_loop(1, count, came_back, 0)
    table = jnp.concatenate([back[expert] for expert in range(count)], axis=0)
    first_pick = jnp.dot(first_ref[...], table, preferred_element_type=jnp.float32)
    second_pick = jnp.dot(second_ref[...], table, preferred_element_type=jnp.float32)
    weights = rw_ref[...]
    mixture = weights[:, 0:1] * first_pick + weights[:, 1:2] * second_pick
    out_ref[...] = (hid_ref[...] + mixture).astype(jnp.bfloat16)

    def sent(step, carry):
        dispatch(step).wait_send()
        giving_back(step).wait_send()
        return carry

    lax.fori_loop(1, count, sent, 0)
    for copy in started:
        copy.wait_send()


def moe(place_t, first, second, route_weights, normed, hidden_state, gate_weight, up_weight, down_weight):
    count = lax.axis_size("sp")
    tokens, width = normed.shape
    inner = gate_weight.shape[2]
    rows = 2 * count // UNITS
    bf16 = jnp.bfloat16
    vmem = pl.BlockSpec(memory_space=pltpu.VMEM)
    hbm = pl.BlockSpec(memory_space=pl.ANY)
    return pl.pallas_call(
        functools.partial(moe_kernel, count),
        out_shape=jax.ShapeDtypeStruct((tokens, width), bf16),
        in_specs=[vmem] * 6 + [hbm] * 3,
        out_specs=vmem,
        scratch_shapes=[
            pltpu.VMEM((width, inner), bf16),
            pltpu.VMEM((width, inner), bf16),
            pltpu.VMEM((inner, width), bf16),
            pltpu.VMEM((count, 2, width), bf16),
            pltpu.VMEM((count, 2, width), bf16),
            pltpu.VMEM((UNITS, RING, RING, rows, width), bf16),
            pltpu.VMEM((UNITS, RING, RING, rows, width), bf16),
            pltpu.VMEM((UNITS, 2, RING // 2, rows, width), bf16),
            pltpu.VMEM((UNITS, 2, RING, rows, width), bf16),
            pltpu.VMEM((UNITS, RING, rows, width), bf16),
            pltpu.VMEM((UNITS, 2, rows // 2, width), bf16),
            pltpu.VMEM((UNITS, 2, rows, width), bf16),
            pltpu.VMEM((count, 2, width), bf16),
            pltpu.VMEM((count, 2, width), bf16),
            pltpu.SemaphoreType.DMA((3,)),
            pltpu.SemaphoreType.DMA((count,)),
            pltpu.SemaphoreType.DMA((count,)),
            pltpu.SemaphoreType.DMA((count,)),
            pltpu.SemaphoreType.DMA((count,)),
            pltpu.SemaphoreType.DMA((UNITS, 16)),
            pltpu.SemaphoreType.DMA((UNITS, 16)),
        ],
        compiler_params=pltpu.CompilerParams(
            collective_id=0, has_side_effects=True, vmem_limit_bytes=60 * 1024 * 1024
        ),
        name="moe",
    )(place_t, first, second, route_weights, normed, hidden_state, gate_weight, up_weight, down_weight)


def local(
    queries,
    keys,
    values,
    sink_logit,
    out_weight,
    residual,
    norm_gain,
    routes,
    route_weights,
    gate_weight,
    up_weight,
    down_weight,
):
    attention = attend_local(queries, keys, values, sink_logit)
    columns = jnp.dot(
        gather_directly(attention, "tp", 1), out_weight, preferred_element_type=jnp.float32
    )
    projected = lax.all_to_all(
        columns.astype(jnp.bfloat16), "tp", split_axis=0, concat_axis=1, tiled=True
    )
    hidden_state = residual.astype(jnp.float32) + projected.astype(jnp.float32)
    inverse = lax.rsqrt(jnp.mean(hidden_state * hidden_state, axis=-1, keepdims=True) + EPS)
    normed = (hidden_state * inverse * norm_gain).astype(jnp.bfloat16)
    sp_count = lax.axis_size("sp")
    tok_rows = residual.shape[0]
    capacity = max(2, 4 * tok_rows // sp_count)
    slot_total = sp_count * capacity
    expert_ids = routes.reshape(-1)
    onehot = (expert_ids[:, None] == jnp.arange(sp_count, dtype=jnp.int32)[None, :]).astype(
        jnp.int32
    )
    earlier = jnp.cumsum(onehot, axis=0) - onehot
    rank = jnp.sum(earlier * onehot, axis=1)
    slots = expert_ids * capacity + rank
    slot_ids = jnp.arange(slot_total, dtype=jnp.int32)
    pairs = slots.reshape(tok_rows, 2)
    first_place = (pairs[:, 0:1] == slot_ids[None, :]).astype(jnp.bfloat16)
    second_place = (pairs[:, 1:2] == slot_ids[None, :]).astype(jnp.bfloat16)
    place_t = (
        (pairs[:, 0][None, :] == slot_ids[:, None]) | (pairs[:, 1][None, :] == slot_ids[:, None])
    ).astype(jnp.bfloat16)
    return moe(
        place_t, first_place, second_place, route_weights, normed, hidden_state,
        gate_weight, up_weight, down_weight,
    )


def solution(mesh):
    in_specs = (
        P("sp", "tp"),
        P("sp", "tp"),
        P("sp", "tp"),
        P("tp"),
        P(None, "tp"),
        P(("sp", "tp"), None),
        P(),
        P(("sp", "tp"), None),
        P(("sp", "tp"), None),
        P("sp", None, "tp"),
        P("sp", None, "tp"),
        P("sp", "tp", None),
    )
    out_specs = P(("sp", "tp"), None)
    return jax.shard_map(local, mesh=mesh, in_specs=in_specs, out_specs=out_specs, check_vma=False)
```

```python
import functools

import jax
import jax.numpy as jnp
from jax import lax
from jax.experimental import pallas as pl
from jax.experimental.pallas import tpu as pltpu
from jax.sharding import PartitionSpec as P

HEADS = 32
KV_HEADS = 16
HEAD = 64
WINDOW = 128
EPS = 1e-06
NEGATIVE = -1e30

UNITS = 4
RING = 4
MESH = pl.DeviceIdType.MESH
BF16 = jnp.bfloat16
F32 = jnp.float32


def remote(src, dst, send_sem, recv_sem, device):
    return pltpu.make_async_remote_copy(
        src_ref=src, dst_ref=dst, send_sem=send_sem, recv_sem=recv_sem, device_id=device, device_id_type=MESH
    )


def contract_last(a, b):
    return lax.dot_general(a, b, (((1,), (1,)), ((), ())), preferred_element_type=F32)


def kernel(
    count,
    q_ref, kt_ref, vt_ref, sink_ref, w_ref, res_ref, gain_ref, routes_ref, rw_ref, wg_hbm, wu_hbm, wd_hbm,
    out_ref,
    wg, wu, wd, k_ext, v_ext, w_rows, attn, hid,
    sending, arrived, x_all, p_all, half_s, full_s, sums, half_f, full_f,
    pp_all, phalf_s, pfull_s, psums, phalf_f, pfull_f,
    back_send, back,
    w_sem, h_send, h_recv, o_send, o_recv, d_send, d_recv, b_send, b_recv, g_send, g_recv, r_send, r_recv, p_send, p_recv,
):
    me = lax.axis_index("sp")
    tp = lax.axis_index("tp")
    peers = RING * RING
    ty, tx = tp // RING, lax.rem(tp, RING)
    spot = {"x": tx, "y": ty}
    rows = 2 * count // UNITS
    per = count // UNITS
    tokens, width = hid.shape
    length = q_ref.shape[0]
    groups = length // WINDOW

    def shifted(pos, delta):
        return lax.rem(pos + (delta + RING), RING)

    def near(axis, delta):
        if axis == "x":
            return (me, ty * RING + shifted(tx, delta))
        return (me, shifted(ty, delta) * RING + tx)

    weight_copies = [
        pltpu.make_async_copy(wg_hbm.at[0], wg, w_sem.at[0]),
        pltpu.make_async_copy(wu_hbm.at[0], wu, w_sem.at[1]),
        pltpu.make_async_copy(wd_hbm.at[0], wd, w_sem.at[2]),
    ]
    for copy in weight_copies:
        copy.start()

    barrier = pltpu.get_barrier_semaphore()

    def greet_sp(step, carry):
        pl.semaphore_signal(barrier, inc=1, device_id=(lax.rem(me + step, count), tp), device_id_type=MESH)
        return carry

    def greet_tp(step, carry):
        pl.semaphore_signal(barrier, inc=1, device_id=(me, lax.rem(tp + step, peers)), device_id_type=MESH)
        return carry

    lax.fori_loop(1, count, greet_sp, 0)
    lax.fori_loop(1, peers, greet_tp, 0)

    t_row = lax.broadcasted_iota(jnp.int32, (tokens, tokens), 0)
    t_col = lax.broadcasted_iota(jnp.int32, (tokens, tokens), 1)

    def as_column(row):
        spread = jnp.where(t_row == t_col, jnp.broadcast_to(row, (tokens, tokens)), 0.0)
        return jnp.sum(spread, axis=1, keepdims=True)

    named = [routes_ref[a : a + 1, :].astype(F32) for a in range(2)]
    named_column = [as_column(row) for row in named]
    slot = []
    for row in named:
        rank = jnp.zeros((1, tokens), F32)
        for column in named_column:
            same = (column == row) & (t_row < t_col)
            rank = rank + jnp.sum(jnp.where(same, 1.0, 0.0), axis=0, keepdims=True)
        slot.append(2.0 * row + rank)
    slot_down = lax.broadcasted_iota(jnp.int32, (2 * count, tokens), 0).astype(F32)
    slot_across = lax.broadcasted_iota(jnp.int32, (tokens, 2 * count), 1).astype(F32)
    placed = jnp.where((slot_down == slot[0]) | (slot_down == slot[1]), 1.0, 0.0).astype(BF16)
    picks = [jnp.where(slot_across == as_column(row), 1.0, 0.0).astype(BF16) for row in slot]
    route_weight = [as_column(rw_ref[a : a + 1, :]) for a in range(2)]

    k_ext[:, WINDOW : WINDOW + length] = kt_ref[...]
    v_ext[:, WINDOW : WINDOW + length] = vt_ref[...]
    block = pl.ds(pl.multiple_of(tp * WINDOW, WINDOW), WINDOW)
    w_rows[:, block] = w_ref[block, :]

    pl.semaphore_wait(barrier, count - 1 + peers - 1)

    right, left = lax.rem(me + 1, count), lax.rem(me + count - 1, count)
    halo = []
    for i, (own, ext) in enumerate(((kt_ref, k_ext), (vt_ref, v_ext))):
        halo.append(
            remote(
                own.at[:, length - WINDOW : length], ext.at[:, 0:WINDOW], h_send.at[2 * i], h_recv.at[2 * i], (right, tp)
            )
        )
        halo.append(
            remote(
                own.at[:, 0:WINDOW], ext.at[:, WINDOW + length : 2 * WINDOW + length],
                h_send.at[2 * i + 1], h_recv.at[2 * i + 1], (left, tp),
            )
        )
    for copy in halo:
        copy.start()

    def columns_to(step):
        to = lax.rem(tp + step, peers)
        return remote(
            w_ref.at[pl.ds(pl.multiple_of(to * WINDOW, WINDOW), WINDOW), :],
            w_rows.at[:, block],
            o_send.at[step], o_recv.at[step], (me, to),
        )

    def send_columns(step, carry):
        columns_to(step).start()
        return carry

    lax.fori_loop(1, peers, send_columns, 0)

    for copy in halo:
        copy.wait_recv()
    row_i = lax.broadcasted_iota(jnp.int32, (WINDOW, 3 * WINDOW), 0)
    col_j = lax.broadcasted_iota(jnp.int32, (WINDOW, 3 * WINDOW), 1)
    close = (col_j >= row_i) & (col_j <= row_i + 2 * WINDOW)
    for n in range(groups):
        position = me * length + (n - 1) * WINDOW + col_j
        valid = close & (position >= 0) & (position < length * count)
        band = slice(n * WINDOW, (n + 3) * WINDOW)
        for r in range(HEADS // KV_HEADS):
            query = q_ref[n * WINDOW : (n + 1) * WINDOW, r * HEAD : (r + 1) * HEAD]
            scores = jnp.dot(query, k_ext[:, band], preferred_element_type=F32) * HEAD ** (-0.5)
            sink = jnp.full((WINDOW, 1), sink_ref[r], F32)
            masked = jnp.where(valid, scores, NEGATIVE)
            top = jnp.maximum(jnp.max(masked, axis=-1, keepdims=True), sink)
            probs = jnp.exp(masked - top)
            denom = jnp.sum(probs, axis=-1, keepdims=True) + jnp.exp(sink - top)
            weights = (probs / denom).astype(BF16)
            attn[n * WINDOW : (n + 1) * WINDOW, r * HEAD : (r + 1) * HEAD] = contract_last(
                weights, v_ext[:, band]
            ).astype(BF16)

    def columns_here(step, carry):
        source = lax.rem(tp + (peers - step), peers)
        place = w_rows.at[:, pl.ds(pl.multiple_of(source * WINDOW, WINDOW), WINDOW)]
        remote(place, place, o_send.at[step], o_recv.at[step], (me, tp)).wait_recv()
        return carry

    lax.fori_loop(1, peers, columns_here, 0)

    started = []

    class Reduction:
        def __init__(self, axes, parts, hs, fs, total, hf, ff, send_sem, recv_sem):
            self.first, self.second = axes
            self.f, self.s = spot[self.first], spot[self.second]
            self.parts, self.hs, self.fs, self.total, self.hf, self.ff = parts, hs, fs, total, hf, ff
            self.send_sem, self.recv_sem = send_sem, recv_sem
            self.rows = parts.shape[2]
            self.half = self.rows // 2

        def copy(self, number, src, dst, axis, delta):
            return remote(src, dst, self.send_sem.at[number], self.recv_sem.at[number], near(axis, delta))

        def send(self, number, src, dst, axis, delta):
            copy = self.copy(number, src, dst, axis, delta)
            copy.start()
            started.append(copy)

        def landed(self, number, dst):
            self.copy(number, dst, dst, "x", 1).wait_recv()

        def at(self, k):
            return shifted(self.f, (0, -1, 1, 2)[k])

        def begin(self):
            h, far = self.half, shifted(self.s, 2)
            for k in (3, 1, 2, 0):
                src = self.parts.at[far, self.at(k)]
                self.send(2 * k, src.at[0:h], self.hs.at[0, k], self.second, 1)
                self.send(2 * k + 1, src.at[h : 2 * h], self.hs.at[1, k], self.second, -1)

        def relay(self, k):
            h, fk = self.half, self.at(k)
            up, down = shifted(self.s, 1), shifted(self.s, -1)
            self.landed(2 * k, self.hs.at[0, k])
            self.parts[up, fk, 0:h] = (self.parts[up, fk, 0:h].astype(F32) + self.hs[0, k].astype(F32)).astype(BF16)
            self.send(8 + 2 * k, self.parts.at[up, fk], self.fs.at[0, k], self.second, 1)
            self.landed(2 * k + 1, self.hs.at[1, k])
            self.parts[down, fk, h : 2 * h] = (
                self.parts[down, fk, h : 2 * h].astype(F32) + self.hs[1, k].astype(F32)
            ).astype(BF16)
            self.send(9 + 2 * k, self.parts.at[down, fk], self.fs.at[1, k], self.second, -1)

        def summed(self, k):
            self.landed(8 + 2 * k, self.fs.at[0, k])
            self.landed(9 + 2 * k, self.fs.at[1, k])
            return self.parts[self.s, self.at(k)].astype(F32) + self.fs[0, k].astype(F32) + self.fs[1, k].astype(F32)

        def turn(self):
            h = self.half
            self.total[3] = self.summed(3).astype(BF16)
            self.send(16, self.total.at[3, 0:h], self.hf.at[0], self.first, 1)
            self.send(17, self.total.at[3, h : 2 * h], self.hf.at[1], self.first, -1)

        def cross(self):
            h = self.half
            high = self.summed(2)
            self.landed(16, self.hf.at[0])
            self.total[2, 0:h] = (high[0:h] + self.hf[0].astype(F32)).astype(BF16)
            self.total[2, h : 2 * h] = high[h:].astype(BF16)
            self.send(18, self.total.at[2], self.ff.at[0], self.first, 1)
            low = self.summed(1)
            self.landed(17, self.hf.at[1])
            self.total[1, 0:h] = low[0:h].astype(BF16)
            self.total[1, h : 2 * h] = (low[h:] + self.hf[1].astype(F32)).astype(BF16)
            self.send(19, self.total.at[1], self.ff.at[1], self.first, -1)

        def finish(self):
            own = self.summed(0)
            self.landed(18, self.ff.at[0])
            self.landed(19, self.ff.at[1])
            return own + self.ff[0].astype(F32) + self.ff[1].astype(F32)

    part_width = width // 2
    step_width = min(512, part_width)
    for n in range(0, width, step_width):
        part = jnp.dot(attn[...], w_rows[:, n : n + step_width], preferred_element_type=F32).astype(BF16)
        color, at = n // part_width, n % part_width
        for t in range(peers):
            y, x = t // RING, t % RING
            i, j = (y, x) if color == 0 else (x, y)
            pp_all[color, i, j, :, at : at + step_width] = part[t * tokens : (t + 1) * tokens, :]

    projections = [
        Reduction(
            (("x", "y"), ("y", "x"))[c], pp_all.at[c], phalf_s.at[c], pfull_s.at[c], psums.at[c], phalf_f.at[c],
            pfull_f.at[c], p_send.at[c], p_recv.at[c],
        )
        for c in range(2)
    ]
    for red in projections:
        red.begin()
    for k in (3, 1, 2, 0):
        for red in projections:
            red.relay(k)
    for red in projections:
        red.turn()
    for red in projections:
        red.cross()
    for c, red in enumerate(projections):
        columns = slice(c * part_width, (c + 1) * part_width)
        hid[:, columns] = res_ref[:, columns].astype(F32) + red.finish()

    hidden_state = hid[...]
    inverse = lax.rsqrt(jnp.mean(hidden_state * hidden_state, axis=-1, keepdims=True) + EPS)
    normed = (hidden_state * inverse * gain_ref[...]).astype(BF16)
    slots = jnp.dot(placed, normed, preferred_element_type=F32).astype(BF16)
    for expert in range(count):
        sending[expert] = slots[2 * expert : 2 * expert + 2, :]

    def dispatch(step):
        to = lax.rem(me + step, count)
        return remote(
            sending.at[to], arrived.at[count - step], d_send.at[step], d_recv.at[count - step], (to, tp)
        )

    def dispatch_pair(step, carry):
        dispatch(step).start()
        dispatch(count - step).start()
        return carry

    lax.fori_loop(1, count // 2, dispatch_pair, 0)
    dispatch(count // 2).start()
    arrived[0] = sending[me]

    class Gather:
        def __init__(self, unit, axes):
            self.unit = unit
            self.first, self.second = axes
            self.f, self.s = spot[self.first], spot[self.second]
            self.x = x_all.at[unit]
            self.half = rows // 2

        def copy(self, number, src, dst, axis, delta):
            return remote(src, dst, g_send.at[self.unit, number], g_recv.at[self.unit, number], near(axis, delta))

        def send(self, number, ref, axis, delta):
            copy = self.copy(number, ref, ref, axis, delta)
            copy.start()
            started.append(copy)

        def landed(self, number, dst):
            self.copy(number, dst, dst, "x", 1).wait_recv()

        def at(self, k):
            return shifted(self.f, (0, -1, 1, 2)[k])

        def across(self, k):
            own = self.x.at[self.s, self.at(k)]
            self.send(4 + 2 * k, own, self.second, 1)
            self.send(5 + 2 * k, own, self.second, -1)

        def begin(self):
            pieces = []
            for j in range(per):
                o = self.unit * per + j
                if o:
                    remote(arrived.at[o], arrived.at[o], d_send.at[o], d_recv.at[o], (me, tp)).wait_recv()
                pieces.append(arrived[o])
            for j in range(per):
                self.x[self.s, self.f, 2 * j : 2 * j + 2, :] = pieces[j]
            own = self.x.at[self.s, self.f]
            self.send(0, own, self.first, 1)
            self.send(1, own, self.first, -1)
            self.across(0)

        def along(self):
            h = self.half
            low, high = self.x.at[self.s, self.at(1)], self.x.at[self.s, self.at(2)]
            self.landed(0, low)
            self.send(2, low.at[0:h], self.first, 1)
            self.landed(1, high)
            self.send(3, high.at[h : 2 * h], self.first, -1)
            self.across(1)
            self.across(2)

        def turn(self):
            h = self.half
            far = self.x.at[self.s, self.at(3)]
            self.landed(2, far.at[0:h])
            self.landed(3, far.at[h : 2 * h])
            self.across(3)

        def relay(self, k):
            h, fk = self.half, self.at(k)
            low, high = self.x.at[shifted(self.s, -1), fk], self.x.at[shifted(self.s, 1), fk]
            self.landed(4 + 2 * k, low)
            self.send(12 + 2 * k, low.at[0:h], self.second, 1)
            self.landed(5 + 2 * k, high)
            self.send(13 + 2 * k, high.at[h : 2 * h], self.second, -1)

        def complete(self):
            h, far = self.half, shifted(self.s, 2)
            for k in (0, 1, 2, 3):
                place = self.x.at[far, self.at(k)]
                self.landed(12 + 2 * k, place.at[0:h])
                self.landed(13 + 2 * k, place.at[h : 2 * h])

    axes = [("x", "y"), ("x", "y"), ("y", "x"), ("y", "x")]
    gathers = [Gather(u, axes[u]) for u in range(UNITS)]
    reductions = [
        Reduction(
            axes[u], p_all.at[u], half_s.at[u], full_s.at[u], sums.at[u], half_f.at[u], full_f.at[u],
            r_send.at[u], r_recv.at[u],
        )
        for u in range(UNITS)
    ]

    def mlp(u):
        gathers[u].complete()
        flat = x_all[u].reshape(peers * rows, width)
        gate = contract_last(flat, wg[...])
        upward = contract_last(flat, wu[...])
        hidden = (gate / (1.0 + jnp.exp(-gate)) * upward).astype(BF16)
        step = min(512, width)
        for n in range(0, width, step):
            part = jnp.dot(hidden, wd[:, n : n + step], preferred_element_type=F32)
            p_all[u, :, :, :, n : n + step] = part.astype(BF16).reshape(RING, RING, rows, step)

    def giving_back(o):
        to = lax.rem(me + o, count)
        return remote(back_send.at[o], back.at[me], b_send.at[o], b_recv.at[me], (to, tp))

    def give_back(u):
        total = reductions[u].finish().astype(BF16)
        for j in range(per):
            o = u * per + j
            if o:
                back_send[o] = total[2 * j : 2 * j + 2, :]
            else:
                back[me] = total[0:2, :]
        for j in range(per):
            o = u * per + j
            if o:
                giving_back(o).start()

    early, late = (0, 3), (1, 2)
    for u in early:
        gathers[u].begin()
    for u in early:
        gathers[u].along()
    for u in early:
        gathers[u].relay(0)
    for u in early:
        gathers[u].turn()
    for k in (1, 2):
        for u in early:
            gathers[u].relay(k)
    for u in late:
        gathers[u].begin()
    for u in early:
        gathers[u].relay(3)
    for u in late:
        gathers[u].along()
    for u in late:
        gathers[u].relay(0)
    for copy in weight_copies:
        copy.wait()
    mlp(0)
    reductions[0].begin()
    for u in late:
        gathers[u].turn()
    mlp(3)
    reductions[3].begin()
    for k in (1, 2, 3):
        for u in late:
            gathers[u].relay(k)
    for k in (3, 1, 2, 0):
        for u in early:
            reductions[u].relay(k)
    mlp(1)
    reductions[1].begin()
    for u in early:
        reductions[u].turn()
    mlp(2)
    reductions[2].begin()
    for u in early:
        reductions[u].cross()
    for k in (3, 1, 2, 0):
        for u in late:
            reductions[u].relay(k)
    for u in early:
        give_back(u)
    for u in late:
        reductions[u].turn()
    for u in late:
        reductions[u].cross()
    for u in late:
        give_back(u)

    def came_back(step, carry):
        sender = lax.rem(me + step, count)
        remote(back.at[sender], back.at[sender], b_send.at[step], b_recv.at[sender], (me, tp)).wait_recv()
        return carry

    lax.fori_loop(1, count, came_back, 0)
    table = jnp.concatenate([back[expert] for expert in range(count)], axis=0)
    mixture = route_weight[0] * jnp.dot(picks[0], table, preferred_element_type=F32)
    mixture = mixture + route_weight[1] * jnp.dot(picks[1], table, preferred_element_type=F32)
    out_ref[...] = hid[...] + mixture

    def sent(step, carry):
        dispatch(step).wait_send()
        giving_back(step).wait_send()
        return carry

    lax.fori_loop(1, count, sent, 0)

    def columns_sent(step, carry):
        columns_to(step).wait_send()
        return carry

    lax.fori_loop(1, peers, columns_sent, 0)
    for copy in halo + started:
        copy.wait_send()


def local(
    queries, keys, values, sink_logit, out_weight, residual, norm_gain, routes, route_weights,
    gate_weight, up_weight, down_weight,
):
    count = lax.axis_size("sp")
    tokens, width = residual.shape
    length, kv = keys.shape
    inner = gate_weight.shape[2]
    heads = queries.shape[1]
    rows = 2 * count // UNITS
    half = rows // 2
    vmem = pl.BlockSpec(memory_space=pltpu.VMEM)
    smem = pl.BlockSpec(memory_space=pltpu.SMEM)
    hbm = pl.BlockSpec(memory_space=pl.ANY)
    dma = pltpu.SemaphoreType.DMA

    def reduction_buffers(units, tall, wide):
        return [
            pltpu.VMEM((units, RING, RING, tall, wide), BF16),
            pltpu.VMEM((units, 2, RING, tall // 2, wide), BF16),
            pltpu.VMEM((units, 2, RING, tall, wide), BF16),
            pltpu.VMEM((units, RING, tall, wide), BF16),
            pltpu.VMEM((units, 2, tall // 2, wide), BF16),
            pltpu.VMEM((units, 2, tall, wide), BF16),
        ]

    out = pl.pallas_call(
        functools.partial(kernel, count),
        out_shape=jax.ShapeDtypeStruct((tokens, width), F32),
        in_specs=[vmem, vmem, vmem, smem, vmem, vmem, vmem, vmem, vmem, hbm, hbm, hbm],
        out_specs=vmem,
        scratch_shapes=[
            pltpu.VMEM((inner, width), BF16),
            pltpu.VMEM((inner, width), BF16),
            pltpu.VMEM((inner, width), BF16),
            pltpu.VMEM((kv, length + 2 * WINDOW), BF16),
            pltpu.VMEM((kv, length + 2 * WINDOW), BF16),
            pltpu.VMEM((heads, width), BF16),
            pltpu.VMEM((length, heads), BF16),
            pltpu.VMEM((tokens, width), F32),
            pltpu.VMEM((count, 2, width), BF16),
            pltpu.VMEM((count, 2, width), BF16),
            pltpu.VMEM((UNITS, RING, RING, rows, width), BF16),
            *reduction_buffers(UNITS, rows, width),
            *reduction_buffers(2, tokens, width // 2),
            pltpu.VMEM((count, 2, width), BF16),
            pltpu.VMEM((count, 2, width), BF16),
            dma((3,)),
            dma((4,)),
            dma((4,)),
            dma((RING * RING,)),
            dma((RING * RING,)),
            dma((count,)),
            dma((count,)),
            dma((count,)),
            dma((count,)),
            dma((UNITS, 20)),
            dma((UNITS, 20)),
            dma((UNITS, 20)),
            dma((UNITS, 20)),
            dma((2, 20)),
            dma((2, 20)),
        ],
        compiler_params=pltpu.CompilerParams(
            collective_id=0, has_side_effects=True, vmem_limit_bytes=60 * 1024 * 1024
        ),
        name="layer",
    )(
        queries, keys.T, values.T, sink_logit, out_weight, residual, norm_gain.reshape(1, width), routes.T,
        route_weights.T, jnp.swapaxes(gate_weight, 1, 2), jnp.swapaxes(up_weight, 1, 2), down_weight,
    )
    return out.astype(BF16)


def solution(mesh):
    in_specs = (
        P("sp", "tp"),
        P("sp", "tp"),
        P("sp", "tp"),
        P("tp"),
        P(None, "tp"),
        P(("sp", "tp"), None),
        P(),
        P(("sp", "tp"), None),
        P(("sp", "tp"), None),
        P("sp", None, "tp"),
        P("sp", None, "tp"),
        P("sp", "tp", None),
    )
    out_specs = P(("sp", "tp"), None)
    return jax.shard_map(local, mesh=mesh, in_specs=in_specs, out_specs=out_specs, check_vma=False)
```

```python
import functools

import jax
import jax.numpy as jnp
from jax import lax
from jax.experimental import pallas as pl
from jax.experimental.pallas import tpu as pltpu
from jax.sharding import PartitionSpec as P

HEADS = 32
KV_HEADS = 16
HEAD = 64
WINDOW = 128
EPS = 1e-06
NEGATIVE = -1e30

UNITS = 4
RING = 4
MESH = pl.DeviceIdType.MESH
BF16 = jnp.bfloat16
F32 = jnp.float32


def remote(src, dst, send_sem, recv_sem, device):
    return pltpu.make_async_remote_copy(
        src_ref=src, dst_ref=dst, send_sem=send_sem, recv_sem=recv_sem, device_id=device, device_id_type=MESH
    )


def contract_last(a, b):
    return lax.dot_general(a, b, (((1,), (1,)), ((), ())), preferred_element_type=F32)


def kernel(
    count,
    q_in, kt_in, vt_in, sink_in, w_in, res_in, gain_in, routes_in, rw_in, wg_in, wu_in, wd_in,
    out_ref,
    q_ref, kt_ref, vt_ref, sink_ref, w_ref, res_ref, gain_ref, routes_ref, rw_ref, wg, wu, wd,
    k_ext, v_ext, attn_all, cols, proj,
    sending, arrived, x_all, p_all, half_s, full_s, sums, half_f, full_f, back_send, back,
    in_sem, h_send, h_recv, a_send, a_recv, o_send, o_recv, d_send, d_recv, b_send, b_recv, g_send, g_recv, r_send, r_recv,
):
    me = lax.axis_index("sp")
    tp = lax.axis_index("tp")
    peers = RING * RING
    ty, tx = tp // RING, lax.rem(tp, RING)
    spot = {"x": tx, "y": ty}
    rows = 2 * count // UNITS
    per = count // UNITS
    tokens, width = proj.shape
    length = q_ref.shape[0]
    groups = length // WINDOW

    def shifted(pos, delta):
        return lax.rem(pos + (delta + RING), RING)

    def near(axis, delta):
        if axis == "x":
            return (me, ty * RING + shifted(tx, delta))
        return (me, shifted(ty, delta) * RING + tx)

    barrier = pltpu.get_barrier_semaphore()

    def greet_sp(step, carry):
        pl.semaphore_signal(barrier, inc=1, device_id=(lax.rem(me + step, count), tp), device_id_type=MESH)
        return carry

    def greet_tp(step, carry):
        pl.semaphore_signal(barrier, inc=1, device_id=(me, lax.rem(tp + step, peers)), device_id_type=MESH)
        return carry

    lax.fori_loop(1, count, greet_sp, 0)
    lax.fori_loop(1, peers, greet_tp, 0)

    pairs = [
        (kt_in, kt_ref), (vt_in, vt_ref), (q_in, q_ref), (sink_in, sink_ref), (routes_in, routes_ref), (rw_in, rw_ref),
        (w_in, w_ref), (res_in, res_ref), (gain_in, gain_ref), (wg_in.at[0], wg), (wu_in.at[0], wu), (wd_in.at[0], wd),
    ]
    loads = [pltpu.make_async_copy(src, dst, in_sem.at[i]) for i, (src, dst) in enumerate(pairs)]
    for copy in loads:
        copy.start()
    for copy in loads[:4]:
        copy.wait()
    k_ext[:, WINDOW : WINDOW + length] = kt_ref[...]
    v_ext[:, WINDOW : WINDOW + length] = vt_ref[...]
    pl.semaphore_wait(barrier, count - 1 + peers - 1)

    right, left = lax.rem(me + 1, count), lax.rem(me + count - 1, count)
    for own, ext in ((kt_ref, k_ext), (vt_ref, v_ext)):
        remote(
            own.at[:, length - WINDOW : length], ext.at[:, 0:WINDOW], h_send.at[0], h_recv.at[0], (right, tp)
        ).start()
        remote(
            own.at[:, 0:WINDOW], ext.at[:, WINDOW + length : 2 * WINDOW + length], h_send.at[0], h_recv.at[0], (left, tp)
        ).start()
    halo = remote(k_ext, k_ext, h_send.at[0], h_recv.at[0], (me, tp))
    halo.wait_recv()

    class Gather:
        def __init__(self, blocks, base, axes, send_sem, recv_sem):
            self.blocks, self.base = blocks, base
            self.first, self.second = axes
            self.f, self.s = spot[self.first], spot[self.second]
            self.half = blocks.shape[1] // 2
            self.send_sem, self.recv_sem = send_sem, recv_sem

        def place(self, s, k):
            return self.base + s * RING + shifted(self.f, (0, -1, 1, 2)[k])

        def block(self, s, k):
            return self.blocks.at[self.place(s, k)]

        def send(self, number, ref, axis, delta):
            remote(ref, ref, self.send_sem, self.recv_sem.at[number], near(axis, delta)).start()

        def landed(self, number, ref):
            remote(ref, ref, self.send_sem, self.recv_sem.at[number], near("x", 1)).wait_recv()

        def begin(self):
            own = self.block(self.s, 0)
            self.send(0, own, self.first, 1)
            self.send(1, own, self.first, -1)

        def across(self, k):
            own = self.block(self.s, k)
            self.send(3 + k, own, self.second, 1)
            self.send(3 + k, own, self.second, -1)

        def along(self):
            h = self.half
            low, high = self.block(self.s, 1), self.block(self.s, 2)
            self.landed(0, low)
            self.send(2, low.at[0:h], self.first, 1)
            self.landed(1, high)
            self.send(2, high.at[h : 2 * h], self.first, -1)

        def turn(self):
            self.landed(2, self.block(self.s, 3))
            self.across(3)

        def relay(self, k):
            h = self.half
            low, high = self.block(shifted(self.s, -1), k), self.block(shifted(self.s, 1), k)
            self.landed(3 + k, self.blocks.at[0:2])
            self.send(7, low.at[0:h], self.second, 1)
            self.send(7, high.at[h : 2 * h], self.second, -1)

        def complete(self):
            self.landed(7, self.blocks.at[0:RING])

    orders = [("x", "y"), ("y", "x")]
    attended = [Gather(attn_all, n * peers, orders[n], a_send.at[0], a_recv.at[n]) for n in range(groups)]

    row_i = lax.broadcasted_iota(jnp.int32, (WINDOW, 3 * WINDOW), 0)
    col_j = lax.broadcasted_iota(jnp.int32, (WINDOW, 3 * WINDOW), 1)
    close = (col_j >= row_i) & (col_j <= row_i + 2 * WINDOW)
    for n in range(groups):
        position = me * length + (n - 1) * WINDOW + col_j
        valid = close & (position >= 0) & (position < length * count)
        band = slice(n * WINDOW, (n + 3) * WINDOW)
        for r in range(HEADS // KV_HEADS):
            query = q_ref[n * WINDOW : (n + 1) * WINDOW, r * HEAD : (r + 1) * HEAD]
            scores = jnp.dot(query, k_ext[:, band], preferred_element_type=F32) * HEAD ** (-0.5)
            sink = jnp.full((WINDOW, 1), sink_ref[r], F32)
            masked = jnp.where(valid, scores, NEGATIVE)
            top = jnp.maximum(jnp.max(masked, axis=-1, keepdims=True), sink)
            probs = jnp.exp(masked - top)
            denom = jnp.sum(probs, axis=-1, keepdims=True) + jnp.exp(sink - top)
            weights = (probs / denom).astype(BF16)
            attn_all[attended[n].place(attended[n].s, 0), :, r * HEAD : (r + 1) * HEAD] = contract_last(
                weights, v_ext[:, band]
            ).astype(BF16)
        attended[n].begin()
    for part in attended:
        part.across(0)

    for copy in loads[4:9]:
        copy.wait()
    t_row = lax.broadcasted_iota(jnp.int32, (tokens, tokens), 0)
    t_col = lax.broadcasted_iota(jnp.int32, (tokens, tokens), 1)

    def as_column(row):
        spread = jnp.where(t_row == t_col, jnp.broadcast_to(row, (tokens, tokens)), 0.0)
        return jnp.sum(spread, axis=1, keepdims=True)

    named = [routes_ref[a : a + 1, :].astype(F32) for a in range(2)]
    named_column = [as_column(row) for row in named]
    slot = []
    for row in named:
        rank = jnp.zeros((1, tokens), F32)
        for column in named_column:
            same = (column == row) & (t_row < t_col)
            rank = rank + jnp.sum(jnp.where(same, 1.0, 0.0), axis=0, keepdims=True)
        slot.append(2.0 * row + rank)
    slot_down = lax.broadcasted_iota(jnp.int32, (2 * count, tokens), 0).astype(F32)
    slot_across = lax.broadcasted_iota(jnp.int32, (tokens, 2 * count), 1).astype(F32)
    placed = jnp.where((slot_down == slot[0]) | (slot_down == slot[1]), 1.0, 0.0).astype(BF16)
    picks = [jnp.where(slot_across == as_column(row), 1.0, 0.0).astype(BF16) for row in slot]
    route_weight = [as_column(rw_ref[a : a + 1, :]) for a in range(2)]

    def both(items, *stages):
        for name, *given in stages:
            for item in items:
                getattr(item, name)(*given)

    both(
        attended, ("along",), ("across", 1), ("across", 2), ("relay", 0), ("turn",), ("relay", 1), ("relay", 2),
        ("relay", 3), ("complete",),
    )

    for n in range(groups):
        ys = [(t // RING, t % RING) if n == 0 else (t % RING, t // RING) for t in range(peers)]
        joined = jnp.concatenate([attn_all[n * peers + i * RING + j] for i, j in ys], axis=1)
        cols[n * WINDOW : (n + 1) * WINDOW, :] = jnp.dot(
            joined, w_ref[...], preferred_element_type=F32
        ).astype(BF16)
    own_columns = pl.ds(pl.multiple_of(tp * WINDOW, WINDOW), WINDOW)

    def rows_to(step, carry):
        to = lax.rem(tp + step, peers)
        remote(
            cols.at[pl.ds(pl.multiple_of(to * tokens, tokens), tokens), :], proj.at[:, own_columns],
            o_send.at[0], o_recv.at[0], (me, to),
        ).start()
        return carry

    lax.fori_loop(1, peers, rows_to, 0)
    proj[:, own_columns] = cols[pl.ds(pl.multiple_of(tp * tokens, tokens), tokens), :]
    others = proj.at[:, 0 : (peers - 1) * WINDOW]
    exchanged = remote(others, others, o_send.at[0], o_recv.at[0], (me, tp))
    exchanged.wait_recv()

    hidden_state = res_ref[...].astype(F32) + proj[...].astype(F32)
    inverse = lax.rsqrt(jnp.mean(hidden_state * hidden_state, axis=-1, keepdims=True) + EPS)
    normed = (hidden_state * inverse * gain_ref[...]).astype(BF16)
    slots = jnp.dot(placed, normed, preferred_element_type=F32).astype(BF16)
    for expert in range(count):
        sending[expert] = slots[2 * expert : 2 * expert + 2, :]

    def dispatch(step):
        to = lax.rem(me + step, count)
        remote(
            sending.at[to], arrived.at[count - step], d_send.at[0], d_recv.at[(count - step) // per], (to, tp)
        ).start()

    def dispatch_pair(step, carry):
        dispatch(step)
        dispatch(count - step)
        return carry

    lax.fori_loop(1, count // 2, dispatch_pair, 0)
    dispatch(count // 2)
    arrived[0] = sending[me]

    class Reduction:
        def __init__(self, unit, axes):
            self.first, self.second = axes
            self.f, self.s = spot[self.first], spot[self.second]
            self.parts, self.hs, self.fs = p_all.at[unit], half_s.at[unit], full_s.at[unit]
            self.total, self.hf, self.ff = sums.at[unit], half_f.at[unit], full_f.at[unit]
            self.recv_sem = r_recv.at[unit]

        def send(self, number, src, dst, axis, delta):
            remote(src, dst, r_send.at[0], self.recv_sem.at[number], near(axis, delta)).start()

        def landed(self, number, ref):
            remote(ref, ref, r_send.at[0], self.recv_sem.at[number], near("x", 1)).wait_recv()

        def at(self, k):
            return shifted(self.f, (0, -1, 1, 2)[k])

        def begin(self):
            h, far = rows // 2, shifted(self.s, 2)
            for k in (3, 1, 2, 0):
                src = self.parts.at[far, self.at(k)]
                self.send(k, src.at[0:h], self.hs.at[k, 0], self.second, 1)
                self.send(k, src.at[h:rows], self.hs.at[k, 1], self.second, -1)

        def relay(self, k):
            h, fk = rows // 2, self.at(k)
            up, down = shifted(self.s, 1), shifted(self.s, -1)
            self.landed(k, self.hs.at[k])
            self.parts[up, fk, 0:h] = (self.parts[up, fk, 0:h].astype(F32) + self.hs[k, 0].astype(F32)).astype(BF16)
            self.send(4 + k, self.parts.at[up, fk], self.fs.at[k, 0], self.second, 1)
            self.parts[down, fk, h:rows] = (
                self.parts[down, fk, h:rows].astype(F32) + self.hs[k, 1].astype(F32)
            ).astype(BF16)
            self.send(4 + k, self.parts.at[down, fk], self.fs.at[k, 1], self.second, -1)

        def summed(self, k):
            self.landed(4 + k, self.fs.at[k])
            return self.parts[self.s, self.at(k)].astype(F32) + self.fs[k, 0].astype(F32) + self.fs[k, 1].astype(F32)

        def turn(self):
            h = rows // 2
            self.total[3] = self.summed(3).astype(BF16)
            self.send(8, self.total.at[3, 0:h], self.hf.at[0], self.first, 1)
            self.send(9, self.total.at[3, h:rows], self.hf.at[1], self.first, -1)

        def cross(self):
            h = rows // 2
            high = self.summed(2)
            self.landed(8, self.hf.at[0])
            self.total[2, 0:h] = (high[0:h] + self.hf[0].astype(F32)).astype(BF16)
            self.total[2, h:rows] = high[h:].astype(BF16)
            self.send(10, self.total.at[2], self.ff.at[0], self.first, 1)
            low = self.summed(1)
            self.landed(9, self.hf.at[1])
            self.total[1, 0:h] = low[0:h].astype(BF16)
            self.total[1, h:rows] = (low[h:] + self.hf[1].astype(F32)).astype(BF16)
            self.send(10, self.total.at[1], self.ff.at[1], self.first, -1)

        def finish(self):
            own = self.summed(0)
            self.landed(10, self.ff)
            return own + self.ff[0].astype(F32) + self.ff[1].astype(F32)

    axes = [orders[0], orders[0], orders[1], orders[1]]
    gathers = [Gather(x_all, u * peers, axes[u], g_send.at[0], g_recv.at[u]) for u in range(UNITS)]
    reductions = [Reduction(u, axes[u]) for u in range(UNITS)]

    def rows_here(u):
        first = 1 if u == 0 else 0
        region = arrived.at[u * per + first : (u + 1) * per]
        remote(region, region, d_send.at[0], d_recv.at[u], (me, tp)).wait_recv()
        place = gathers[u].place(gathers[u].s, 0)
        for j in range(per):
            x_all[place, 2 * j : 2 * j + 2, :] = arrived[u * per + j]

    held = {}

    def mlp_up(u):
        gathers[u].complete()
        flat = x_all[u * peers : (u + 1) * peers].reshape(peers * rows, width)
        gate = contract_last(flat, wg[...])
        upward = contract_last(flat, wu[...])
        held[u] = (gate / (1.0 + jnp.exp(-gate)) * upward).astype(BF16)

    def mlp_down(u):
        step = min(512, width)
        for n in range(0, width, step):
            part = jnp.dot(held[u], wd[:, n : n + step], preferred_element_type=F32)
            p_all[u, :, :, :, n : n + step] = part.astype(BF16).reshape(RING, RING, rows, step)

    def give_back(u):
        total = reductions[u].finish().astype(BF16)
        for j in range(per):
            o = u * per + j
            if o:
                back_send[o] = total[2 * j : 2 * j + 2, :]
            else:
                back[me] = total[0:2, :]
        for j in range(per):
            o = u * per + j
            if o:
                remote(
                    back_send.at[o], back.at[me], b_send.at[0], b_recv.at[0], (lax.rem(me + o, count), tp)
                ).start()

    early = [gathers[0], gathers[3]]
    late = [gathers[1], gathers[2]]
    for u in (0, 3):
        rows_here(u)
        gathers[u].begin()
    both(early, ("across", 0), ("along",), ("across", 1), ("across", 2), ("relay", 0), ("turn",), ("relay", 1), ("relay", 2))
    for u in (1, 2):
        rows_here(u)
        gathers[u].begin()
    both(late, ("across", 0))
    both(early, ("relay", 3))
    both(late, ("along",), ("across", 1), ("across", 2))
    for copy in loads[9:]:
        copy.wait()
    mlp_up(0)
    both(late, ("relay", 0))
    mlp_down(0)
    reductions[0].begin()
    both(late, ("turn",))
    mlp_up(3)
    both(late, ("relay", 1))
    mlp_down(3)
    reductions[3].begin()
    both(late, ("relay", 2), ("relay", 3))
    for k in (3, 1, 2, 0):
        reductions[0].relay(k)
    mlp_up(1)
    mlp_down(1)
    reductions[1].begin()
    for k in (3, 1, 2, 0):
        reductions[3].relay(k)
    reductions[0].turn()
    mlp_up(2)
    mlp_down(2)
    reductions[2].begin()
    reductions[3].turn()
    for k in (3, 1, 2, 0):
        reductions[1].relay(k)
    reductions[0].cross()
    reductions[3].cross()
    for k in (3, 1, 2, 0):
        reductions[2].relay(k)
    give_back(0)
    give_back(3)
    reductions[1].turn()
    reductions[2].turn()
    reductions[1].cross()
    reductions[2].cross()
    give_back(1)
    give_back(2)

    from_others = back.at[0 : count - 1]
    returned = remote(from_others, from_others, b_send.at[0], b_recv.at[0], (me, tp))
    returned.wait_recv()
    table = jnp.concatenate([back[expert] for expert in range(count)], axis=0)
    mixture = route_weight[0] * jnp.dot(picks[0], table, preferred_element_type=F32)
    mixture = mixture + route_weight[1] * jnp.dot(picks[1], table, preferred_element_type=F32)
    out_ref[...] = hidden_state + mixture

    returned.wait_send()
    dispatched = sending.at[0 : count - 1]
    remote(dispatched, dispatched, d_send.at[0], b_recv.at[0], (me, tp)).wait_send()
    exchanged.wait_send()
    halo.wait_send()
    sent = attn_all.at[0 : groups * (peers - 1)]
    remote(sent, sent, a_send.at[0], b_recv.at[0], (me, tp)).wait_send()
    sent = x_all.at[0 : UNITS * (peers - 1)]
    remote(sent, sent, g_send.at[0], b_recv.at[0], (me, tp)).wait_send()
    remote(sent, sent, r_send.at[0], b_recv.at[0], (me, tp)).wait_send()


def local(
    queries, keys, values, sink_logit, out_weight, residual, norm_gain, routes, route_weights,
    gate_weight, up_weight, down_weight,
):
    count = lax.axis_size("sp")
    tokens, width = residual.shape
    length, kv = keys.shape
    inner = gate_weight.shape[2]
    heads = queries.shape[1]
    rows = 2 * count // UNITS
    half = rows // 2
    groups = length // WINDOW
    peers = RING * RING
    dma = pltpu.SemaphoreType.DMA
    given = (
        queries, keys.T, values.T, sink_logit, out_weight, residual, norm_gain.reshape(1, width), routes.T,
        route_weights.T, jnp.swapaxes(gate_weight, 1, 2), jnp.swapaxes(up_weight, 1, 2), down_weight,
    )
    held = [pltpu.VMEM(a.shape, a.dtype) for a in given[:9]] + [pltpu.VMEM((inner, width), BF16)] * 3
    held[3] = pltpu.SMEM(sink_logit.shape, F32)
    out = pl.pallas_call(
        functools.partial(kernel, count),
        out_shape=jax.ShapeDtypeStruct((tokens, width), F32),
        in_specs=[pl.BlockSpec(memory_space=pl.ANY)] * len(given),
        out_specs=pl.BlockSpec(memory_space=pltpu.VMEM),
        scratch_shapes=[
            *held,
            pltpu.VMEM((kv, length + 2 * WINDOW), BF16),
            pltpu.VMEM((kv, length + 2 * WINDOW), BF16),
            pltpu.VMEM((groups * peers, WINDOW, heads), BF16),
            pltpu.VMEM((length, heads), BF16),
            pltpu.VMEM((tokens, width), BF16),
            pltpu.VMEM((count, 2, width), BF16),
            pltpu.VMEM((count, 2, width), BF16),
            pltpu.VMEM((UNITS * peers, rows, width), BF16),
            pltpu.VMEM((UNITS, RING, RING, rows, width), BF16),
            pltpu.VMEM((UNITS, RING, 2, half, width), BF16),
            pltpu.VMEM((UNITS, RING, 2, rows, width), BF16),
            pltpu.VMEM((UNITS, RING, rows, width), BF16),
            pltpu.VMEM((UNITS, 2, half, width), BF16),
            pltpu.VMEM((UNITS, 2, rows, width), BF16),
            pltpu.VMEM((count, 2, width), BF16),
            pltpu.VMEM((count, 2, width), BF16),
            dma((len(given),)),
            dma((1,)),
            dma((1,)),
            dma((1,)),
            dma((groups, 8)),
            dma((1,)),
            dma((1,)),
            dma((1,)),
            dma((UNITS,)),
            dma((1,)),
            dma((1,)),
            dma((1,)),
            dma((UNITS, 8)),
            dma((1,)),
            dma((UNITS, 11)),
        ],
        compiler_params=pltpu.CompilerParams(
            collective_id=0, has_side_effects=True, vmem_limit_bytes=60 * 1024 * 1024
        ),
        name="layer",
    )(*given)
    return out.astype(BF16)


def solution(mesh):
    in_specs = (
        P("sp", "tp"),
        P("sp", "tp"),
        P("sp", "tp"),
        P("tp"),
        P(None, "tp"),
        P(("sp", "tp"), None),
        P(),
        P(("sp", "tp"), None),
        P(("sp", "tp"), None),
        P("sp", None, "tp"),
        P("sp", None, "tp"),
        P("sp", "tp", None),
    )
    out_specs = P(("sp", "tp"), None)
    return jax.shard_map(local, mesh=mesh, in_specs=in_specs, out_specs=out_specs, check_vma=False)
```

```python
import functools

import jax
import jax.numpy as jnp
from jax import lax
from jax.experimental import pallas as pl
from jax.experimental.pallas import tpu as pltpu
from jax.sharding import PartitionSpec as P

HEADS = 32
KV_HEADS = 16
HEAD = 64
WINDOW = 128
EPS = 1e-06
NEGATIVE = -1e30

UNITS = 8
RING = 4
ORDER = (
    (0, 0), (0, 1), (1, 0), (0, 2), (0, 3), (0, 4), (0, 5), (1, 1), (2, 0), (0, 6), (1, 2), (1, 3), (3, 0), (2, 1),
    (1, 4), (0, 7), (1, 5), (1, 6), (2, 2), (0, 8), (2, 3), (3, 1), (2, 4), (2, 5), (3, 2), (1, 7), (2, 6), (3, 3),
    (1, 8), (1, 9), (3, 4), (0, 9), (3, 5), (2, 7), (3, 6), (1, 10), (2, 8), (2, 9), (1, 11), (1, 12), (1, 13),
    (2, 10), (1, 14), (2, 11), (2, 12), (3, 7), (2, 13), (3, 8), (2, 14), (1, 15), (3, 9), (0, 10), (2, 15), (1, 16),
    (3, 10), (3, 11), (3, 12), (3, 13), (2, 16), (3, 14), (0, 11), (0, 12), (0, 13), (0, 14), (3, 15), (0, 15),
    (3, 16), (0, 16),
)
MESH = pl.DeviceIdType.MESH
BF16 = jnp.bfloat16
F32 = jnp.float32


def remote(src, dst, send_sem, recv_sem, device):
    return pltpu.make_async_remote_copy(
        src_ref=src, dst_ref=dst, send_sem=send_sem, recv_sem=recv_sem, device_id=device, device_id_type=MESH
    )


def contract_last(a, b):
    return lax.dot_general(a, b, (((1,), (1,)), ((), ())), preferred_element_type=F32)


def kernel(
    count,
    q_in, kt_in, vt_in, sink_in, w_in, res_in, gain_in, routes_in, rw_in, wg_in, wu_in, wd_in,
    out_ref,
    q_ref, kt_ref, vt_ref, sink_ref, w_ref, res_ref, gain_ref, routes_ref, rw_ref, wg, wu, wd,
    k_ext, v_ext, attn_all, cols, proj,
    sending, arrived, x_all, p_all, half_s, full_s, sums, half_f, full_f, back_send, back,
    in_sem, h_send, h_recv, a_send, a_recv, o_send, o_recv, d_send, d_recv, b_send, b_recv, g_send, g_recv, r_send, r_recv,
):
    me = lax.axis_index("sp")
    tp = lax.axis_index("tp")
    peers = RING * RING
    ty, tx = tp // RING, lax.rem(tp, RING)
    spot = {"x": tx, "y": ty}
    rows = 2 * count // UNITS
    per = count // UNITS
    tokens, width = proj.shape
    length = q_ref.shape[0]
    groups = length // WINDOW

    def shifted(pos, delta):
        return lax.rem(pos + (delta + RING), RING)

    def near(axis, delta):
        if axis == "x":
            return (me, ty * RING + shifted(tx, delta))
        return (me, shifted(ty, delta) * RING + tx)

    barrier = pltpu.get_barrier_semaphore()

    def greet_sp(step, carry):
        pl.semaphore_signal(barrier, inc=1, device_id=(lax.rem(me + step, count), tp), device_id_type=MESH)
        return carry

    def greet_tp(step, carry):
        pl.semaphore_signal(barrier, inc=1, device_id=(me, lax.rem(tp + step, peers)), device_id_type=MESH)
        return carry

    lax.fori_loop(1, count, greet_sp, 0)
    lax.fori_loop(1, peers, greet_tp, 0)

    pairs = [
        (kt_in, kt_ref), (vt_in, vt_ref), (q_in, q_ref), (sink_in, sink_ref), (routes_in, routes_ref), (rw_in, rw_ref),
        (w_in, w_ref), (res_in, res_ref), (gain_in, gain_ref), (wg_in.at[0], wg), (wu_in.at[0], wu), (wd_in.at[0], wd),
    ]
    loads = [pltpu.make_async_copy(src, dst, in_sem.at[i]) for i, (src, dst) in enumerate(pairs)]
    for copy in loads:
        copy.start()
    for copy in loads[:4]:
        copy.wait()
    k_ext[:, WINDOW : WINDOW + length] = kt_ref[...]
    v_ext[:, WINDOW : WINDOW + length] = vt_ref[...]
    pl.semaphore_wait(barrier, count - 1 + peers - 1)

    right, left = lax.rem(me + 1, count), lax.rem(me + count - 1, count)
    for own, ext in ((kt_ref, k_ext), (vt_ref, v_ext)):
        remote(
            own.at[:, length - WINDOW : length], ext.at[:, 0:WINDOW], h_send.at[0], h_recv.at[0], (right, tp)
        ).start()
        remote(
            own.at[:, 0:WINDOW], ext.at[:, WINDOW + length : 2 * WINDOW + length], h_send.at[0], h_recv.at[0], (left, tp)
        ).start()
    halo = remote(k_ext, k_ext, h_send.at[0], h_recv.at[0], (me, tp))
    halo.wait_recv()

    class Gather:
        def __init__(self, blocks, base, axes, cut, send_sem, recv_sem):
            self.blocks, self.base, self.cut = blocks, base, cut
            self.first, self.second = axes
            self.f, self.s = spot[self.first], spot[self.second]
            self.send_sem, self.recv_sem = send_sem, recv_sem

        def place(self, s, k):
            return self.base + s * RING + shifted(self.f, (0, -1, 1, 2)[k])

        def block(self, s, k):
            return self.blocks.at[self.place(s, k)]

        def part(self, ref, which):
            if self.cut == 0:
                h = ref.shape[0] // 2
                return ref.at[which * h : (which + 1) * h]
            h = ref.shape[1] // 2
            return ref.at[:, which * h : (which + 1) * h]

        def send(self, number, ref, axis, delta):
            remote(ref, ref, self.send_sem, self.recv_sem.at[number], near(axis, delta)).start()

        def landed(self, number, ref):
            remote(ref, ref, self.send_sem, self.recv_sem.at[number], near("x", 1)).wait_recv()

        def begin(self):
            own = self.block(self.s, 0)
            self.send(0, own, self.first, 1)
            self.send(1, own, self.first, -1)

        def across(self, k):
            own = self.block(self.s, k)
            self.send(3 + k, own, self.second, 1)
            self.send(3 + k, own, self.second, -1)

        def along(self):
            low, high = self.block(self.s, 1), self.block(self.s, 2)
            self.landed(0, low)
            self.send(2, self.part(low, 0), self.first, 1)
            self.landed(1, high)
            self.send(2, self.part(high, 1), self.first, -1)

        def turn(self):
            self.landed(2, self.block(self.s, 3))
            self.across(3)

        def relay(self, k):
            low, high = self.block(shifted(self.s, -1), k), self.block(shifted(self.s, 1), k)
            self.landed(3 + k, self.blocks.at[0:2])
            self.send(7, self.part(low, 0), self.second, 1)
            self.send(7, self.part(high, 1), self.second, -1)

        def complete(self):
            self.landed(7, self.blocks.at[0:RING])

    orders = [("x", "y"), ("y", "x")]
    attended = [Gather(attn_all, n * peers, orders[n], 0, a_send.at[0], a_recv.at[n]) for n in range(groups)]

    row_i = lax.broadcasted_iota(jnp.int32, (WINDOW, 3 * WINDOW), 0)
    col_j = lax.broadcasted_iota(jnp.int32, (WINDOW, 3 * WINDOW), 1)
    close = (col_j >= row_i) & (col_j <= row_i + 2 * WINDOW)
    for n in range(groups):
        position = me * length + (n - 1) * WINDOW + col_j
        valid = close & (position >= 0) & (position < length * count)
        band = slice(n * WINDOW, (n + 3) * WINDOW)
        for r in range(HEADS // KV_HEADS):
            query = q_ref[n * WINDOW : (n + 1) * WINDOW, r * HEAD : (r + 1) * HEAD]
            scores = jnp.dot(query, k_ext[:, band], preferred_element_type=F32) * HEAD ** (-0.5)
            sink = jnp.full((WINDOW, 1), sink_ref[r], F32)
            masked = jnp.where(valid, scores, NEGATIVE)
            top = jnp.maximum(jnp.max(masked, axis=-1, keepdims=True), sink)
            probs = jnp.exp(masked - top)
            denom = jnp.sum(probs, axis=-1, keepdims=True) + jnp.exp(sink - top)
            weights = (probs / denom).astype(BF16)
            attn_all[attended[n].place(attended[n].s, 0), :, r * HEAD : (r + 1) * HEAD] = contract_last(
                weights, v_ext[:, band]
            ).astype(BF16)
        attended[n].begin()
    for part in attended:
        part.across(0)

    for copy in loads[4:9]:
        copy.wait()
    t_row = lax.broadcasted_iota(jnp.int32, (tokens, tokens), 0)
    t_col = lax.broadcasted_iota(jnp.int32, (tokens, tokens), 1)

    def as_column(row):
        spread = jnp.where(t_row == t_col, jnp.broadcast_to(row, (tokens, tokens)), 0.0)
        return jnp.sum(spread, axis=1, keepdims=True)

    named = [routes_ref[a : a + 1, :].astype(F32) for a in range(2)]
    named_column = [as_column(row) for row in named]
    slot = []
    for row in named:
        rank = jnp.zeros((1, tokens), F32)
        for column in named_column:
            same = (column == row) & (t_row < t_col)
            rank = rank + jnp.sum(jnp.where(same, 1.0, 0.0), axis=0, keepdims=True)
        slot.append(2.0 * row + rank)
    slot_down = lax.broadcasted_iota(jnp.int32, (2 * count, tokens), 0).astype(F32)
    slot_across = lax.broadcasted_iota(jnp.int32, (tokens, 2 * count), 1).astype(F32)
    placed = jnp.where((slot_down == slot[0]) | (slot_down == slot[1]), 1.0, 0.0).astype(BF16)
    picks = [jnp.where(slot_across == as_column(row), 1.0, 0.0).astype(BF16) for row in slot]
    route_weight = [as_column(rw_ref[a : a + 1, :]) for a in range(2)]

    def both(items, *stages):
        for name, *given in stages:
            for item in items:
                getattr(item, name)(*given)

    both(
        attended, ("along",), ("across", 1), ("across", 2), ("relay", 0), ("turn",), ("relay", 1), ("relay", 2),
        ("relay", 3), ("complete",),
    )

    for n in range(groups):
        ys = [(t // RING, t % RING) if n == 0 else (t % RING, t // RING) for t in range(peers)]
        joined = jnp.concatenate([attn_all[n * peers + i * RING + j] for i, j in ys], axis=1)
        cols[n * WINDOW : (n + 1) * WINDOW, :] = jnp.dot(
            joined, w_ref[...], preferred_element_type=F32
        ).astype(BF16)
    own_columns = pl.ds(pl.multiple_of(tp * WINDOW, WINDOW), WINDOW)

    def rows_to(step, carry):
        to = lax.rem(tp + step, peers)
        remote(
            cols.at[pl.ds(pl.multiple_of(to * tokens, tokens), tokens), :], proj.at[:, own_columns],
            o_send.at[0], o_recv.at[0], (me, to),
        ).start()
        return carry

    lax.fori_loop(1, peers, rows_to, 0)
    proj[:, own_columns] = cols[pl.ds(pl.multiple_of(tp * tokens, tokens), tokens), :]
    others = proj.at[:, 0 : (peers - 1) * WINDOW]
    exchanged = remote(others, others, o_send.at[0], o_recv.at[0], (me, tp))
    exchanged.wait_recv()

    hidden_state = res_ref[...].astype(F32) + proj[...].astype(F32)
    inverse = lax.rsqrt(jnp.mean(hidden_state * hidden_state, axis=-1, keepdims=True) + EPS)
    normed = (hidden_state * inverse * gain_ref[...]).astype(BF16)
    slots = jnp.dot(placed, normed, preferred_element_type=F32).astype(BF16)
    for expert in range(count):
        sending[expert] = slots[2 * expert : 2 * expert + 2, :]

    def dispatch(step):
        to = lax.rem(me + step, count)
        remote(
            sending.at[to], arrived.at[count - step], d_send.at[0], d_recv.at[(count - step) // per], (to, tp)
        ).start()

    pairs = [(u, UNITS - 1 - u) for u in range(UNITS // 2)]
    pairs = [pairs[0], *pairs[2:], pairs[1]]

    def dispatch_pair(step, carry):
        dispatch(step + 1)
        dispatch(count - step)
        return carry

    for low, _ in pairs:
        if low == 0:
            dispatch(1)
        lax.fori_loop(max(low * per, 1), (low + 1) * per, dispatch_pair, 0)
    arrived[0] = sending[me]

    class Reduction:
        def __init__(self, unit, axes):
            self.first, self.second = axes
            self.f, self.s = spot[self.first], spot[self.second]
            self.parts, self.hs, self.fs = p_all.at[unit], half_s.at[unit], full_s.at[unit]
            self.total, self.hf, self.ff = sums.at[unit], half_f.at[unit], full_f.at[unit]
            self.recv_sem = r_recv.at[unit]

        def send(self, number, src, dst, axis, delta):
            remote(src, dst, r_send.at[0], self.recv_sem.at[number], near(axis, delta)).start()

        def landed(self, number, ref):
            remote(ref, ref, r_send.at[0], self.recv_sem.at[number], near("x", 1)).wait_recv()

        def at(self, k):
            return shifted(self.f, (0, -1, 1, 2)[k])

        def begin(self):
            h, far = width // 2, shifted(self.s, 2)
            for k in (3, 1, 2, 0):
                src = self.parts.at[far, self.at(k)]
                self.send(k, src.at[:, 0:h], self.hs.at[k, 0], self.second, 1)
                self.send(k, src.at[:, h:width], self.hs.at[k, 1], self.second, -1)

        def relay(self, k):
            h, fk = width // 2, self.at(k)
            up, down = shifted(self.s, 1), shifted(self.s, -1)
            self.landed(k, self.hs.at[k])
            self.parts[up, fk, :, 0:h] = (
                self.parts[up, fk, :, 0:h].astype(F32) + self.hs[k, 0].astype(F32)
            ).astype(BF16)
            self.send(4 + k, self.parts.at[up, fk], self.fs.at[k, 0], self.second, 1)
            self.parts[down, fk, :, h:width] = (
                self.parts[down, fk, :, h:width].astype(F32) + self.hs[k, 1].astype(F32)
            ).astype(BF16)
            self.send(4 + k, self.parts.at[down, fk], self.fs.at[k, 1], self.second, -1)

        def summed(self, k):
            self.landed(4 + k, self.fs.at[k])
            return self.parts[self.s, self.at(k)].astype(F32) + self.fs[k, 0].astype(F32) + self.fs[k, 1].astype(F32)

        def turn(self):
            h = width // 2
            self.total[3] = self.summed(3).astype(BF16)
            self.send(8, self.total.at[3, :, 0:h], self.hf.at[0], self.first, 1)
            self.send(9, self.total.at[3, :, h:width], self.hf.at[1], self.first, -1)

        def cross(self):
            h = width // 2
            high = self.summed(2)
            self.landed(8, self.hf.at[0])
            self.total[2, :, 0:h] = (high[:, 0:h] + self.hf[0].astype(F32)).astype(BF16)
            self.total[2, :, h:width] = high[:, h:].astype(BF16)
            self.send(10, self.total.at[2], self.ff.at[0], self.first, 1)
            low = self.summed(1)
            self.landed(9, self.hf.at[1])
            self.total[1, :, 0:h] = low[:, 0:h].astype(BF16)
            self.total[1, :, h:width] = (low[:, h:] + self.hf[1].astype(F32)).astype(BF16)
            self.send(10, self.total.at[1], self.ff.at[1], self.first, -1)

        def finish(self):
            own = self.summed(0)
            self.landed(10, self.ff)
            return own + self.ff[0].astype(F32) + self.ff[1].astype(F32)

    axes = [orders[2 * u // UNITS] for u in range(UNITS)]
    gathers = [Gather(x_all, u * peers, axes[u], 1, g_send.at[0], g_recv.at[u]) for u in range(UNITS)]
    reductions = [Reduction(u, axes[u]) for u in range(UNITS)]

    def rows_here(u):
        first = 1 if u == 0 else 0
        region = arrived.at[u * per + first : (u + 1) * per]
        remote(region, region, d_send.at[0], d_recv.at[u], (me, tp)).wait_recv()
        place = gathers[u].place(gathers[u].s, 0)
        for j in range(per):
            x_all[place, 2 * j : 2 * j + 2, :] = arrived[u * per + j]

    held = {}

    def mlp_up(pair):
        for u in pair:
            gathers[u].complete()
        flat = jnp.concatenate(
            [x_all[u * peers : (u + 1) * peers].reshape(peers * rows, width) for u in pair], axis=0
        )
        gate = contract_last(flat, wg[...])
        upward = contract_last(flat, wu[...])
        held[pair] = (gate / (1.0 + jnp.exp(-gate)) * upward).astype(BF16)

    def mlp_down(pair):
        step = min(512, width)
        for n in range(0, width, step):
            part = jnp.dot(held[pair], wd[:, n : n + step], preferred_element_type=F32)
            for i, u in enumerate(pair):
                block = part[i * peers * rows : (i + 1) * peers * rows].reshape(RING, RING, rows, step)
                p_all[u, :, :, :, n : n + step] = block.astype(BF16)

    def give_back(u):
        total = reductions[u].finish().astype(BF16)
        for j in range(per):
            o = u * per + j
            if o:
                back_send[o] = total[2 * j : 2 * j + 2, :]
            else:
                back[me] = total[0:2, :]
        for j in range(per):
            o = u * per + j
            if o:
                remote(
                    back_send.at[o], back.at[me], b_send.at[0], b_recv.at[0], (lax.rem(me + o, count), tp)
                ).start()

    for copy in loads[9:]:
        copy.wait()

    def enter(pair):
        for u in pair:
            rows_here(u)
            gathers[u].begin()
        both([gathers[u] for u in pair], ("across", 0))

    def sideways(pair):
        both([gathers[u] for u in pair], ("along",), ("across", 1), ("across", 2))

    def gather_step(name, *given):
        return lambda pair: both([gathers[u] for u in pair], (name, *given))

    def reduce_step(name, *given):
        return lambda pair: both([reductions[u] for u in pair], (name, *given))

    def leave(pair):
        for u in pair:
            give_back(u)

    steps = [
        enter, sideways, gather_step("relay", 0), gather_step("turn"), gather_step("relay", 1), gather_step("relay", 2),
        gather_step("relay", 3), mlp_up, mlp_down, reduce_step("begin"), reduce_step("relay", 3),
        reduce_step("relay", 1), reduce_step("relay", 2), reduce_step("relay", 0), reduce_step("turn"),
        reduce_step("cross"), leave,
    ]
    for i, step in ORDER:
        steps[step](pairs[i])

    from_others = back.at[0 : count - 1]
    returned = remote(from_others, from_others, b_send.at[0], b_recv.at[0], (me, tp))
    returned.wait_recv()
    table = jnp.concatenate([back[expert] for expert in range(count)], axis=0)
    mixture = route_weight[0] * jnp.dot(picks[0], table, preferred_element_type=F32)
    mixture = mixture + route_weight[1] * jnp.dot(picks[1], table, preferred_element_type=F32)
    out_ref[...] = hidden_state + mixture

    returned.wait_send()
    dispatched = sending.at[0 : count - 1]
    remote(dispatched, dispatched, d_send.at[0], b_recv.at[0], (me, tp)).wait_send()
    exchanged.wait_send()
    halo.wait_send()
    sent = attn_all.at[0 : groups * (peers - 1)]
    remote(sent, sent, a_send.at[0], b_recv.at[0], (me, tp)).wait_send()
    sent = x_all.at[0 : UNITS * (peers - 1)]
    remote(sent, sent, g_send.at[0], b_recv.at[0], (me, tp)).wait_send()
    remote(sent, sent, r_send.at[0], b_recv.at[0], (me, tp)).wait_send()


def local(
    queries, keys, values, sink_logit, out_weight, residual, norm_gain, routes, route_weights,
    gate_weight, up_weight, down_weight,
):
    count = lax.axis_size("sp")
    tokens, width = residual.shape
    length, kv = keys.shape
    inner = gate_weight.shape[2]
    heads = queries.shape[1]
    rows = 2 * count // UNITS
    groups = length // WINDOW
    peers = RING * RING
    dma = pltpu.SemaphoreType.DMA
    given = (
        queries, keys.T, values.T, sink_logit, out_weight, residual, norm_gain.reshape(1, width), routes.T,
        route_weights.T, jnp.swapaxes(gate_weight, 1, 2), jnp.swapaxes(up_weight, 1, 2), down_weight,
    )
    held = [pltpu.VMEM(a.shape, a.dtype) for a in given[:9]] + [pltpu.VMEM((inner, width), BF16)] * 3
    held[3] = pltpu.SMEM(sink_logit.shape, F32)
    out = pl.pallas_call(
        functools.partial(kernel, count),
        out_shape=jax.ShapeDtypeStruct((tokens, width), F32),
        in_specs=[pl.BlockSpec(memory_space=pl.ANY)] * len(given),
        out_specs=pl.BlockSpec(memory_space=pltpu.VMEM),
        scratch_shapes=[
            *held,
            pltpu.VMEM((kv, length + 2 * WINDOW), BF16),
            pltpu.VMEM((kv, length + 2 * WINDOW), BF16),
            pltpu.VMEM((groups * peers, WINDOW, heads), BF16),
            pltpu.VMEM((length, heads), BF16),
            pltpu.VMEM((tokens, width), BF16),
            pltpu.VMEM((count, 2, width), BF16),
            pltpu.VMEM((count, 2, width), BF16),
            pltpu.VMEM((UNITS * peers, rows, width), BF16),
            pltpu.VMEM((UNITS, RING, RING, rows, width), BF16),
            pltpu.VMEM((UNITS, RING, 2, rows, width // 2), BF16),
            pltpu.VMEM((UNITS, RING, 2, rows, width), BF16),
            pltpu.VMEM((UNITS, RING, rows, width), BF16),
            pltpu.VMEM((UNITS, 2, rows, width // 2), BF16),
            pltpu.VMEM((UNITS, 2, rows, width), BF16),
            pltpu.VMEM((count, 2, width), BF16),
            pltpu.VMEM((count, 2, width), BF16),
            dma((len(given),)),
            dma((1,)),
            dma((1,)),
            dma((1,)),
            dma((groups, 8)),
            dma((1,)),
            dma((1,)),
            dma((1,)),
            dma((UNITS,)),
            dma((1,)),
            dma((1,)),
            dma((1,)),
            dma((UNITS, 8)),
            dma((1,)),
            dma((UNITS, 11)),
        ],
        compiler_params=pltpu.CompilerParams(
            collective_id=0, has_side_effects=True, vmem_limit_bytes=60 * 1024 * 1024
        ),
        name="layer",
    )(*given)
    return out.astype(BF16)


def solution(mesh):
    in_specs = (
        P("sp", "tp"),
        P("sp", "tp"),
        P("sp", "tp"),
        P("tp"),
        P(None, "tp"),
        P(("sp", "tp"), None),
        P(),
        P(("sp", "tp"), None),
        P(("sp", "tp"), None),
        P("sp", None, "tp"),
        P("sp", None, "tp"),
        P("sp", "tp", None),
    )
    out_specs = P(("sp", "tp"), None)
    return jax.shard_map(local, mesh=mesh, in_specs=in_specs, out_specs=out_specs, check_vma=False)
```

```python
import functools

import jax
import jax.numpy as jnp
from jax import lax
from jax.experimental import pallas as pl
from jax.experimental.pallas import tpu as pltpu
from jax.sharding import PartitionSpec as P

HEADS = 32
KV_HEADS = 16
HEAD = 64
WINDOW = 128
EPS = 1e-06
NEGATIVE = -1e30

UNITS = 8
RING = 4
ORDER = (
    (0, 0), (0, 1), (1, 0), (0, 2), (0, 3), (0, 4), (0, 5), (1, 1), (2, 0), (0, 6), (1, 2), (1, 3), (3, 0), (2, 1),
    (1, 4), (0, 7), (1, 5), (1, 6), (2, 2), (0, 8), (2, 3), (3, 1), (2, 4), (2, 5), (3, 2), (1, 7), (2, 6), (3, 3),
    (1, 8), (1, 9), (3, 4), (0, 9), (3, 5), (2, 7), (3, 6), (1, 10), (2, 8), (2, 9), (1, 11), (1, 12), (1, 13),
    (2, 10), (1, 14), (2, 11), (2, 12), (3, 7), (2, 13), (3, 8), (2, 14), (1, 15), (3, 9), (0, 10), (2, 15), (1, 16),
    (3, 10), (3, 11), (3, 12), (3, 13), (2, 16), (3, 14), (0, 11), (0, 12), (0, 13), (0, 14), (3, 15), (0, 15),
    (3, 16), (0, 16),
)
MESH = pl.DeviceIdType.MESH
BF16 = jnp.bfloat16
F32 = jnp.float32


def remote(src, dst, send_sem, recv_sem, device):
    return pltpu.make_async_remote_copy(
        src_ref=src, dst_ref=dst, send_sem=send_sem, recv_sem=recv_sem, device_id=device, device_id_type=MESH
    )


def contract_last(a, b):
    return lax.dot_general(a, b, (((1,), (1,)), ((), ())), preferred_element_type=F32)


def kernel(
    count,
    q_in, kt_in, vt_in, sink_in, w_in, res_in, gain_in, routes_in, rw_in, wg_in, wu_in, wd_in,
    out_ref,
    q_ref, kt_ref, vt_ref, sink_ref, w_ref, res_ref, gain_ref, routes_ref, rw_ref, wg, wu, wd,
    k_ext, v_ext, w_all, attended, shares, joined, rows_out, proj,
    sending, arrived, x_all, p_all, half_s, full_s, sums, half_f, full_f, back_send, back,
    in_sem, h_send, h_recv, w_send, w_recv, a_send, a_recv, s_send, s_recv, o_send, o_recv, d_send, d_recv, b_send, b_recv, g_send, g_recv, r_send, r_recv,
):
    me = lax.axis_index("sp")
    tp = lax.axis_index("tp")
    peers = RING * RING
    ty, tx = tp // RING, lax.rem(tp, RING)
    spot = {"x": tx, "y": ty}
    rows = 2 * count // UNITS
    per = count // UNITS
    tokens, width = res_ref.shape
    length = q_ref.shape[0]
    orders = [("x", "y"), ("y", "x")]
    colors = range(2)
    part = tokens // 2
    groups = length // WINDOW

    def shifted(pos, delta):
        return lax.rem(pos + (delta + RING), RING)

    def near(axis, delta):
        if axis == "x":
            return (me, ty * RING + shifted(tx, delta))
        return (me, shifted(ty, delta) * RING + tx)

    barrier = pltpu.get_barrier_semaphore()

    def greet_sp(step, carry):
        pl.semaphore_signal(barrier, inc=1, device_id=(lax.rem(me + step, count), tp), device_id_type=MESH)
        return carry

    def greet_tp(step, carry):
        pl.semaphore_signal(barrier, inc=1, device_id=(me, lax.rem(tp + step, peers)), device_id_type=MESH)
        return carry

    lax.fori_loop(1, count, greet_sp, 0)
    lax.fori_loop(1, peers, greet_tp, 0)

    pairs = [
        (kt_in, kt_ref), (vt_in, vt_ref), (q_in, q_ref), (sink_in, sink_ref), (w_in, w_ref), (routes_in, routes_ref),
        (rw_in, rw_ref), (res_in, res_ref), (gain_in, gain_ref), (wg_in.at[0], wg), (wu_in.at[0], wu), (wd_in.at[0], wd),
    ]
    loads = [pltpu.make_async_copy(src, dst, in_sem.at[i]) for i, (src, dst) in enumerate(pairs)]
    for copy in loads:
        copy.start()
    for copy in loads[:5]:
        copy.wait()
    k_ext[:, WINDOW : WINDOW + length] = kt_ref[...]
    v_ext[:, WINDOW : WINDOW + length] = vt_ref[...]
    pl.semaphore_wait(barrier, count - 1 + peers - 1)

    right, left = lax.rem(me + 1, count), lax.rem(me + count - 1, count)
    for own, ext in ((kt_ref, k_ext), (vt_ref, v_ext)):
        remote(
            own.at[:, length - WINDOW : length], ext.at[:, 0:WINDOW], h_send.at[0], h_recv.at[0], (right, tp)
        ).start()
        remote(
            own.at[:, 0:WINDOW], ext.at[:, WINDOW + length : 2 * WINDOW + length], h_send.at[0], h_recv.at[0], (left, tp)
        ).start()
    halo = remote(k_ext, k_ext, h_send.at[0], h_recv.at[0], (me, tp))

    core = lax.rem(me, 2)
    mine = pl.ds(2 * core, 2)

    def head_blocks(c, s):
        return (s, mine) if c == 0 else (mine, s)

    for c in colors:
        second = orders[c][1]
        s = spot[second]
        for delta in (2, 1, -1):
            remote(
                w_ref.at[head_blocks(c, shifted(s, delta))], w_all.at[c, s, mine], w_send.at[0], w_recv.at[0],
                near(second, delta),
            ).start()
        w_all[c, s, mine] = w_ref[head_blocks(c, s)]
    halo.wait_recv()

    class Gather:
        def __init__(self, blocks, base, axes, send_sem, recv_sem):
            self.blocks, self.base = blocks, base
            self.first, self.second = axes
            self.f, self.s = spot[self.first], spot[self.second]
            self.send_sem, self.recv_sem = send_sem, recv_sem

        def place(self, s, k):
            return self.base + s * RING + shifted(self.f, (0, -1, 1, 2)[k])

        def block(self, s, k):
            return self.blocks.at[self.place(s, k)]

        def part(self, ref, which):
            h = ref.shape[1] // 2
            return ref.at[:, which * h : (which + 1) * h]

        def send(self, number, ref, axis, delta):
            remote(ref, ref, self.send_sem, self.recv_sem.at[number], near(axis, delta)).start()

        def landed(self, number, ref):
            remote(ref, ref, self.send_sem, self.recv_sem.at[number], near("x", 1)).wait_recv()

        def begin(self):
            own = self.block(self.s, 0)
            self.send(0, own, self.first, 1)
            self.send(1, own, self.first, -1)

        def across(self, k):
            own = self.block(self.s, k)
            self.send(3 + k, own, self.second, 1)
            self.send(3 + k, own, self.second, -1)

        def along(self):
            low, high = self.block(self.s, 1), self.block(self.s, 2)
            self.landed(0, low)
            self.send(2, self.part(low, 0), self.first, 1)
            self.landed(1, high)
            self.send(2, self.part(high, 1), self.first, -1)

        def turn(self):
            self.landed(2, self.block(self.s, 3))
            self.across(3)

        def relay(self, k):
            low, high = self.block(shifted(self.s, -1), k), self.block(shifted(self.s, 1), k)
            self.landed(3 + k, self.blocks.at[0:2])
            self.send(7, self.part(low, 0), self.second, 1)
            self.send(7, self.part(high, 1), self.second, -1)

        def complete(self):
            self.landed(7, self.blocks.at[0:RING])

    row_i = lax.broadcasted_iota(jnp.int32, (WINDOW, 3 * WINDOW), 0)
    col_j = lax.broadcasted_iota(jnp.int32, (WINDOW, 3 * WINDOW), 1)
    close = (col_j >= row_i) & (col_j <= row_i + 2 * WINDOW)
    for n in range(groups):
        position = me * length + (n - 1) * WINDOW + col_j
        valid = close & (position >= 0) & (position < length * count)
        band = slice(n * WINDOW, (n + 3) * WINDOW)
        for r in range(HEADS // KV_HEADS):
            query = q_ref[n * WINDOW : (n + 1) * WINDOW, r * HEAD : (r + 1) * HEAD]
            scores = jnp.dot(query, k_ext[:, band], preferred_element_type=F32) * HEAD ** (-0.5)
            sink = jnp.full((WINDOW, 1), sink_ref[r], F32)
            masked = jnp.where(valid, scores, NEGATIVE)
            top = jnp.maximum(jnp.max(masked, axis=-1, keepdims=True), sink)
            probs = jnp.exp(masked - top)
            denom = jnp.sum(probs, axis=-1, keepdims=True) + jnp.exp(sink - top)
            weights = (probs / denom).astype(BF16)
            output = contract_last(weights, v_ext[:, band]).reshape(WINDOW // tokens, tokens, HEAD)
            half = WINDOW // 2
            for c in colors:
                attended[c, spot[orders[c][0]], n * half : (n + 1) * half, r * HEAD : (r + 1) * HEAD] = (
                    output[:, c * part : (c + 1) * part].reshape(half, HEAD).astype(BF16)
                )

    for c in colors:
        first = orders[c][0]
        own = attended.at[c, spot[first]]
        for delta in (2, 1, -1):
            remote(own, own, a_send.at[c], a_recv.at[c], near(first, delta)).start()
    fetched = w_all.at[0, 0 : RING - 1]
    remote(fetched, fetched, w_send.at[0], w_recv.at[0], (me, tp)).wait_recv()
    for c in colors:
        half_blocks = w_all.at[c, :, mine]
        remote(half_blocks, half_blocks, w_send.at[1], w_recv.at[1], (me + 1 - 2 * core, tp)).start()

    for copy in loads[5:9]:
        copy.wait()
    t_row = lax.broadcasted_iota(jnp.int32, (tokens, tokens), 0)
    t_col = lax.broadcasted_iota(jnp.int32, (tokens, tokens), 1)

    def as_column(row):
        spread = jnp.where(t_row == t_col, jnp.broadcast_to(row, (tokens, tokens)), 0.0)
        return jnp.sum(spread, axis=1, keepdims=True)

    named = [routes_ref[a : a + 1, :].astype(F32) for a in range(2)]
    named_column = [as_column(row) for row in named]
    slot = []
    for row in named:
        rank = jnp.zeros((1, tokens), F32)
        for column in named_column:
            same = (column == row) & (t_row < t_col)
            rank = rank + jnp.sum(jnp.where(same, 1.0, 0.0), axis=0, keepdims=True)
        slot.append(2.0 * row + rank)
    slot_down = lax.broadcasted_iota(jnp.int32, (2 * count, tokens), 0).astype(F32)
    slot_across = lax.broadcasted_iota(jnp.int32, (tokens, 2 * count), 1).astype(F32)
    placed = jnp.where((slot_down == slot[0]) | (slot_down == slot[1]), 1.0, 0.0).astype(BF16)
    picks = [jnp.where(slot_across == as_column(row), 1.0, 0.0).astype(BF16) for row in slot]
    route_weight = [as_column(rw_ref[a : a + 1, :]) for a in range(2)]

    def both(items, *stages):
        for name, *given in stages:
            for item in items:
                getattr(item, name)(*given)

    handed = w_all.at[0]
    remote(handed, handed, w_send.at[1], w_recv.at[1], (me, tp)).wait_recv()
    for c in colors:
        arriving = attended.at[c, 0 : RING - 1]
        remote(arriving, arriving, a_send.at[c], a_recv.at[c], (me, tp)).wait_recv()
        heads = jnp.concatenate([attended[c, i] for i in range(RING)], axis=1)
        for j in range(RING):
            block = w_all[c, j].reshape(RING * WINDOW, WINDOW)
            share = jnp.dot(heads, block, preferred_element_type=F32)
            for t in range(peers):
                s, f = (t // RING, t % RING) if c == 0 else (t % RING, t // RING)
                shares[c, s, f * part : (f + 1) * part, j * WINDOW : (j + 1) * WINDOW] = share[
                    t * part : (t + 1) * part
                ].astype(BF16)
        second = orders[c][1]
        for delta, place in ((2, 2), (1, 0), (-1, 1)):
            remote(
                shares.at[c, shifted(spot[second], delta)], joined.at[c, place], s_send.at[c], s_recv.at[c],
                near(second, delta),
            ).start()
    for c in colors:
        first, second = orders[c]
        f = spot[first]
        remote(joined.at[c], joined.at[c], s_send.at[c], s_recv.at[c], (me, tp)).wait_recv()
        total = shares[c, spot[second]].astype(F32)
        for i in range(RING - 1):
            total = total + joined[c, i].astype(F32)
        rows_out[c] = total.reshape(RING, part, RING * WINDOW).astype(BF16)
        for delta in (2, 1, -1):
            remote(
                rows_out.at[c, shifted(f, delta)], proj.at[c, f], o_send.at[c], o_recv.at[c], near(first, delta)
            ).start()
        proj[c, f] = rows_out[c, f]
    for c in colors:
        arriving = proj.at[c, 0 : RING - 1]
        remote(arriving, arriving, o_send.at[c], o_recv.at[c], (me, tp)).wait_recv()
    projected = []
    for t in range(peers):
        y, x = t // RING, t % RING
        ends = [proj[0, x, :, y * WINDOW : (y + 1) * WINDOW], proj[1, y, :, x * WINDOW : (x + 1) * WINDOW]]
        projected.append(jnp.concatenate([piece.astype(F32) for piece in ends], axis=0))
    hidden_state = res_ref[...].astype(F32) + jnp.concatenate(projected, axis=1)
    inverse = lax.rsqrt(jnp.mean(hidden_state * hidden_state, axis=-1, keepdims=True) + EPS)
    normed = (hidden_state * inverse * gain_ref[...]).astype(BF16)
    slots = jnp.dot(placed, normed, preferred_element_type=F32).astype(BF16)
    for expert in range(count):
        sending[expert] = slots[2 * expert : 2 * expert + 2, :]

    def dispatch(step):
        to = lax.rem(me + step, count)
        remote(
            sending.at[to], arrived.at[count - step], d_send.at[0], d_recv.at[(count - step) // per], (to, tp)
        ).start()

    pairs = [(u, UNITS - 1 - u) for u in range(UNITS // 2)]
    pairs = [pairs[0], *pairs[2:], pairs[1]]

    def dispatch_pair(step, carry):
        dispatch(step + 1)
        dispatch(count - step)
        return carry

    for low, _ in pairs:
        if low == 0:
            dispatch(1)
        lax.fori_loop(max(low * per, 1), (low + 1) * per, dispatch_pair, 0)
    arrived[0] = sending[me]

    class Reduction:
        def __init__(self, unit, axes):
            self.first, self.second = axes
            self.f, self.s = spot[self.first], spot[self.second]
            self.parts, self.hs, self.fs = p_all.at[unit], half_s.at[unit], full_s.at[unit]
            self.total, self.hf, self.ff = sums.at[unit], half_f.at[unit], full_f.at[unit]
            self.recv_sem = r_recv.at[unit]

        def send(self, number, src, dst, axis, delta):
            remote(src, dst, r_send.at[0], self.recv_sem.at[number], near(axis, delta)).start()

        def landed(self, number, ref):
            remote(ref, ref, r_send.at[0], self.recv_sem.at[number], near("x", 1)).wait_recv()

        def at(self, k):
            return shifted(self.f, (0, -1, 1, 2)[k])

        def begin(self):
            h, far = width // 2, shifted(self.s, 2)
            for k in (3, 1, 2, 0):
                src = self.parts.at[far, self.at(k)]
                self.send(k, src.at[:, 0:h], self.hs.at[k, 0], self.second, 1)
                self.send(k, src.at[:, h:width], self.hs.at[k, 1], self.second, -1)

        def relay(self, k):
            h, fk = width // 2, self.at(k)
            up, down = shifted(self.s, 1), shifted(self.s, -1)
            self.landed(k, self.hs.at[k])
            self.parts[up, fk, :, 0:h] = (
                self.parts[up, fk, :, 0:h].astype(F32) + self.hs[k, 0].astype(F32)
            ).astype(BF16)
            self.send(4 + k, self.parts.at[up, fk], self.fs.at[k, 0], self.second, 1)
            self.parts[down, fk, :, h:width] = (
                self.parts[down, fk, :, h:width].astype(F32) + self.hs[k, 1].astype(F32)
            ).astype(BF16)
            self.send(4 + k, self.parts.at[down, fk], self.fs.at[k, 1], self.second, -1)

        def summed(self, k):
            self.landed(4 + k, self.fs.at[k])
            return self.parts[self.s, self.at(k)].astype(F32) + self.fs[k, 0].astype(F32) + self.fs[k, 1].astype(F32)

        def turn(self):
            h = width // 2
            self.total[3] = self.summed(3).astype(BF16)
            self.send(8, self.total.at[3, :, 0:h], self.hf.at[0], self.first, 1)
            self.send(9, self.total.at[3, :, h:width], self.hf.at[1], self.first, -1)

        def cross(self):
            h = width // 2
            high = self.summed(2)
            self.landed(8, self.hf.at[0])
            self.total[2, :, 0:h] = (high[:, 0:h] + self.hf[0].astype(F32)).astype(BF16)
            self.total[2, :, h:width] = high[:, h:].astype(BF16)
            self.send(10, self.total.at[2], self.ff.at[0], self.first, 1)
            low = self.summed(1)
            self.landed(9, self.hf.at[1])
            self.total[1, :, 0:h] = low[:, 0:h].astype(BF16)
            self.total[1, :, h:width] = (low[:, h:] + self.hf[1].astype(F32)).astype(BF16)
            self.send(10, self.total.at[1], self.ff.at[1], self.first, -1)

        def finish(self):
            own = self.summed(0)
            self.landed(10, self.ff)
            return own + self.ff[0].astype(F32) + self.ff[1].astype(F32)

    axes = [orders[2 * u // UNITS] for u in range(UNITS)]
    gathers = [Gather(x_all, u * peers, axes[u], g_send.at[0], g_recv.at[u]) for u in range(UNITS)]
    reductions = [Reduction(u, axes[u]) for u in range(UNITS)]

    def rows_here(u):
        first = 1 if u == 0 else 0
        region = arrived.at[u * per + first : (u + 1) * per]
        remote(region, region, d_send.at[0], d_recv.at[u], (me, tp)).wait_recv()
        place = gathers[u].place(gathers[u].s, 0)
        for j in range(per):
            x_all[place, 2 * j : 2 * j + 2, :] = arrived[u * per + j]

    held = {}

    def mlp_up(pair):
        for u in pair:
            gathers[u].complete()
        flat = jnp.concatenate(
            [x_all[u * peers : (u + 1) * peers].reshape(peers * rows, width) for u in pair], axis=0
        )
        gate = contract_last(flat, wg[...])
        upward = contract_last(flat, wu[...])
        held[pair] = (gate / (1.0 + jnp.exp(-gate)) * upward).astype(BF16)

    def mlp_down(pair):
        step = min(512, width)
        for n in range(0, width, step):
            part = jnp.dot(held[pair], wd[:, n : n + step], preferred_element_type=F32)
            for i, u in enumerate(pair):
                block = part[i * peers * rows : (i + 1) * peers * rows].reshape(RING, RING, rows, step)
                p_all[u, :, :, :, n : n + step] = block.astype(BF16)

    def give_back(u):
        total = reductions[u].finish().astype(BF16)
        for j in range(per):
            o = u * per + j
            if o:
                back_send[o] = total[2 * j : 2 * j + 2, :]
            else:
                back[me] = total[0:2, :]
        for j in range(per):
            o = u * per + j
            if o:
                remote(
                    back_send.at[o], back.at[me], b_send.at[0], b_recv.at[0], (lax.rem(me + o, count), tp)
                ).start()

    for copy in loads[9:]:
        copy.wait()

    def enter(pair):
        for u in pair:
            rows_here(u)
            gathers[u].begin()
        both([gathers[u] for u in pair], ("across", 0))

    def sideways(pair):
        both([gathers[u] for u in pair], ("along",), ("across", 1), ("across", 2))

    def gather_step(name, *given):
        return lambda pair: both([gathers[u] for u in pair], (name, *given))

    def reduce_step(name, *given):
        return lambda pair: both([reductions[u] for u in pair], (name, *given))

    def leave(pair):
        for u in pair:
            give_back(u)

    steps = [
        enter, sideways, gather_step("relay", 0), gather_step("turn"), gather_step("relay", 1), gather_step("relay", 2),
        gather_step("relay", 3), mlp_up, mlp_down, reduce_step("begin"), reduce_step("relay", 3),
        reduce_step("relay", 1), reduce_step("relay", 2), reduce_step("relay", 0), reduce_step("turn"),
        reduce_step("cross"), leave,
    ]
    for i, step in ORDER:
        steps[step](pairs[i])

    from_others = back.at[0 : count - 1]
    returned = remote(from_others, from_others, b_send.at[0], b_recv.at[0], (me, tp))
    returned.wait_recv()
    table = jnp.concatenate([back[expert] for expert in range(count)], axis=0)
    mixture = route_weight[0] * jnp.dot(picks[0], table, preferred_element_type=F32)
    mixture = mixture + route_weight[1] * jnp.dot(picks[1], table, preferred_element_type=F32)
    out_ref[...] = hidden_state + mixture

    returned.wait_send()
    dispatched = sending.at[0 : count - 1]
    remote(dispatched, dispatched, d_send.at[0], b_recv.at[0], (me, tp)).wait_send()
    halo.wait_send()
    remote(fetched, fetched, w_send.at[0], b_recv.at[0], (me, tp)).wait_send()
    remote(handed, handed, w_send.at[1], b_recv.at[0], (me, tp)).wait_send()
    for c in colors:
        sent = attended.at[c, 0 : RING - 1]
        remote(sent, sent, a_send.at[c], b_recv.at[0], (me, tp)).wait_send()
        remote(joined.at[c], joined.at[c], s_send.at[c], b_recv.at[0], (me, tp)).wait_send()
        sent = proj.at[c, 0 : RING - 1]
        remote(sent, sent, o_send.at[c], b_recv.at[0], (me, tp)).wait_send()
    sent = x_all.at[0 : UNITS * (peers - 1)]
    remote(sent, sent, g_send.at[0], b_recv.at[0], (me, tp)).wait_send()
    remote(sent, sent, r_send.at[0], b_recv.at[0], (me, tp)).wait_send()


def local(
    queries, keys, values, sink_logit, out_weight, residual, norm_gain, routes, route_weights,
    gate_weight, up_weight, down_weight,
):
    count = lax.axis_size("sp")
    tokens, width = residual.shape
    length, kv = keys.shape
    inner = gate_weight.shape[2]
    heads = queries.shape[1]
    rows = 2 * count // UNITS
    peers = RING * RING
    dma = pltpu.SemaphoreType.DMA
    given = (
        queries, keys.T, values.T, sink_logit, out_weight.reshape(RING, RING, WINDOW, WINDOW), residual, norm_gain.reshape(1, width), routes.T,
        route_weights.T, jnp.swapaxes(gate_weight, 1, 2), jnp.swapaxes(up_weight, 1, 2), down_weight,
    )
    held = [pltpu.VMEM(a.shape, a.dtype) for a in given[:9]] + [pltpu.VMEM((inner, width), BF16)] * 3
    held[3] = pltpu.SMEM(sink_logit.shape, F32)
    out = pl.pallas_call(
        functools.partial(kernel, count),
        out_shape=jax.ShapeDtypeStruct((tokens, width), F32),
        in_specs=[pl.BlockSpec(memory_space=pl.ANY)] * len(given),
        out_specs=pl.BlockSpec(memory_space=pltpu.VMEM),
        scratch_shapes=[
            *held,
            pltpu.VMEM((kv, length + 2 * WINDOW), BF16),
            pltpu.VMEM((kv, length + 2 * WINDOW), BF16),
            pltpu.VMEM((2, RING, RING, WINDOW, WINDOW), BF16),
            pltpu.VMEM((2, RING, length // 2, heads), BF16),
            pltpu.VMEM((2, RING, RING * tokens // 2, RING * WINDOW), BF16),
            pltpu.VMEM((2, RING - 1, RING * tokens // 2, RING * WINDOW), BF16),
            pltpu.VMEM((2, RING, tokens // 2, RING * WINDOW), BF16),
            pltpu.VMEM((2, RING, tokens // 2, RING * WINDOW), BF16),
            pltpu.VMEM((count, 2, width), BF16),
            pltpu.VMEM((count, 2, width), BF16),
            pltpu.VMEM((UNITS * peers, rows, width), BF16),
            pltpu.VMEM((UNITS, RING, RING, rows, width), BF16),
            pltpu.VMEM((UNITS, RING, 2, rows, width // 2), BF16),
            pltpu.VMEM((UNITS, RING, 2, rows, width), BF16),
            pltpu.VMEM((UNITS, RING, rows, width), BF16),
            pltpu.VMEM((UNITS, 2, rows, width // 2), BF16),
            pltpu.VMEM((UNITS, 2, rows, width), BF16),
            pltpu.VMEM((count, 2, width), BF16),
            pltpu.VMEM((count, 2, width), BF16),
            dma((len(given),)),
            dma((1,)),
            dma((1,)),
            dma((2,)),
            dma((2,)),
            dma((2,)),
            dma((2,)),
            dma((2,)),
            dma((2,)),
            dma((2,)),
            dma((2,)),
            dma((1,)),
            dma((UNITS,)),
            dma((1,)),
            dma((1,)),
            dma((1,)),
            dma((UNITS, 8)),
            dma((1,)),
            dma((UNITS, 11)),
        ],
        compiler_params=pltpu.CompilerParams(
            collective_id=0, has_side_effects=True, vmem_limit_bytes=60 * 1024 * 1024
        ),
        name="layer",
    )(*given)
    return out.astype(BF16)


def solution(mesh):
    in_specs = (
        P("sp", "tp"),
        P("sp", "tp"),
        P("sp", "tp"),
        P("tp"),
        P(None, "tp"),
        P(("sp", "tp"), None),
        P(),
        P(("sp", "tp"), None),
        P(("sp", "tp"), None),
        P("sp", None, "tp"),
        P("sp", None, "tp"),
        P("sp", "tp", None),
    )
    out_specs = P(("sp", "tp"), None)
    return jax.shard_map(local, mesh=mesh, in_specs=in_specs, out_specs=out_specs, check_vma=False)
```

```python
import functools

import jax
import jax.numpy as jnp
from jax import lax
from jax.experimental import pallas as pl
from jax.experimental.pallas import tpu as pltpu
from jax.sharding import PartitionSpec as P

HEADS = 32
KV_HEADS = 16
HEAD = 64
WINDOW = 128
EPS = 1e-06
NEGATIVE = -1e30

UNITS = 8
RING = 4
ORDER = (
    (0, 0), (0, 1), (0, 2), (0, 3), (1, 0), (0, 4), (0, 5), (0, 6), (1, 1), (2, 0), (1, 2), (1, 3), (1, 4), (3, 0),
    (2, 1), (1, 5), (1, 6), (0, 7), (2, 2), (0, 8), (1, 7), (0, 9), (2, 3), (2, 4), (3, 1), (3, 2), (2, 5), (2, 6),
    (3, 3), (1, 8), (2, 7), (3, 4), (1, 9), (3, 5), (1, 10), (3, 6), (0, 10), (2, 8), (1, 11), (3, 7), (2, 9),
    (2, 10), (1, 12), (1, 13), (1, 14), (1, 15), (2, 11), (2, 12), (2, 13), (2, 14), (3, 8), (3, 9), (1, 16), (1, 17),
    (2, 15), (3, 10), (0, 11), (1, 18), (2, 16), (2, 17), (3, 11), (3, 12), (3, 13), (0, 12), (0, 13), (3, 14),
    (2, 18), (3, 15), (3, 16), (3, 17), (0, 14), (0, 15), (0, 16), (0, 17), (3, 18), (0, 18),
)
MESH = pl.DeviceIdType.MESH
BF16 = jnp.bfloat16
F32 = jnp.float32


def remote(src, dst, send_sem, recv_sem, device):
    return pltpu.make_async_remote_copy(
        src_ref=src, dst_ref=dst, send_sem=send_sem, recv_sem=recv_sem, device_id=device, device_id_type=MESH
    )


def contract_last(a, b):
    return lax.dot_general(a, b, (((1,), (1,)), ((), ())), preferred_element_type=F32)


def kernel(
    count,
    q_in, kt_in, vt_in, sink_in, w_in, res_in, gain_in, routes_in, rw_in, wg_in, wu_in, wd_in,
    out_ref,
    q_ref, kt_ref, vt_ref, sink_ref, w_ref, res_ref, gain_ref, routes_ref, rw_ref, wg, wu, wd,
    k_ext, v_ext, w_all, attended, shares, joined, rows_out, proj,
    sending, arrived, x_all, p_all, half_s, full_s, sums, half_f, full_f, back_send, back,
    in_sem, h_send, h_recv, w_send, w_recv, a_send, a_recv, s_send, s_recv, o_send, o_recv, d_send, d_recv, b_send, b_recv, g_send, g_recv, r_send, r_recv,
):
    me = lax.axis_index("sp")
    tp = lax.axis_index("tp")
    peers = RING * RING
    ty, tx = tp // RING, lax.rem(tp, RING)
    spot = {"x": tx, "y": ty}
    rows = 2 * count // UNITS
    per = count // UNITS
    tokens, width = res_ref.shape
    length = q_ref.shape[0]
    orders = [("x", "y"), ("y", "x")]
    colors = range(2)
    part = tokens // 2
    groups = length // WINDOW

    def shifted(pos, delta):
        return lax.rem(pos + (delta + RING), RING)

    def near(axis, delta):
        if axis == "x":
            return (me, ty * RING + shifted(tx, delta))
        return (me, shifted(ty, delta) * RING + tx)

    pairs = [
        (kt_in, kt_ref), (vt_in, vt_ref), (q_in, q_ref), (sink_in, sink_ref), (w_in, w_ref), (routes_in, routes_ref),
        (rw_in, rw_ref), (res_in, res_ref), (gain_in, gain_ref), (wg_in.at[0], wg), (wu_in.at[0], wu), (wd_in.at[0], wd),
    ]
    loads = [pltpu.make_async_copy(src, dst, in_sem.at[i]) for i, (src, dst) in enumerate(pairs)]
    for copy in loads[:5]:
        copy.start()

    barrier = pltpu.get_barrier_semaphore()

    def greet_sp(step, carry):
        pl.semaphore_signal(barrier, inc=1, device_id=(lax.rem(me + step, count), tp), device_id_type=MESH)
        return carry

    def greet_tp(step, carry):
        pl.semaphore_signal(barrier, inc=1, device_id=(me, lax.rem(tp + step, peers)), device_id_type=MESH)
        return carry

    lax.fori_loop(1, count, greet_sp, 0)
    lax.fori_loop(1, peers, greet_tp, 0)

    for copy in loads[5:]:
        copy.start()
    for copy in loads[:5]:
        copy.wait()
    k_ext[:, WINDOW : WINDOW + length] = kt_ref[...]
    v_ext[:, WINDOW : WINDOW + length] = vt_ref[...]
    pl.semaphore_wait(barrier, count - 1 + peers - 1)

    right, left = lax.rem(me + 1, count), lax.rem(me + count - 1, count)
    for own, ext in ((kt_ref, k_ext), (vt_ref, v_ext)):
        remote(
            own.at[:, length - WINDOW : length], ext.at[:, 0:WINDOW], h_send.at[0], h_recv.at[0], (right, tp)
        ).start()
        remote(
            own.at[:, 0:WINDOW], ext.at[:, WINDOW + length : 2 * WINDOW + length], h_send.at[0], h_recv.at[0], (left, tp)
        ).start()
    halo = remote(k_ext, k_ext, h_send.at[0], h_recv.at[0], (me, tp))

    core = lax.rem(me, 2)
    mine = pl.ds(2 * core, 2)

    def head_blocks(c, s):
        return (s, mine) if c == 0 else (mine, s)

    for c in colors:
        second = orders[c][1]
        s = spot[second]
        for delta in (2, 1, -1):
            remote(
                w_ref.at[head_blocks(c, shifted(s, delta))], w_all.at[c, s, mine], w_send.at[0], w_recv.at[0],
                near(second, delta),
            ).start()
        w_all[c, s, mine] = w_ref[head_blocks(c, s)]

    class Gather:
        def __init__(self, blocks, base, axes, direct, send_sem, recv_sem):
            self.blocks, self.base, self.direct = blocks, base, direct
            self.first, self.second = axes
            self.f, self.s = spot[self.first], spot[self.second]
            self.send_sem, self.recv_sem = send_sem, recv_sem

        def place(self, s, k):
            return self.base + s * RING + shifted(self.f, (0, -1, 1, 2)[k])

        def block(self, s, k):
            return self.blocks.at[self.place(s, k)]

        def part(self, ref, which):
            h = ref.shape[1] // 2
            return ref.at[:, which * h : (which + 1) * h]

        def send(self, number, ref, axis, delta):
            remote(ref, ref, self.send_sem, self.recv_sem.at[number], near(axis, delta)).start()

        def landed(self, number, ref):
            remote(ref, ref, self.send_sem, self.recv_sem.at[number], near("x", 1)).wait_recv()

        def begin(self):
            own = self.block(self.s, 0)
            self.send(0, own, self.first, 1)
            self.send(1, own, self.first, -1)
            if self.direct:
                self.send(2, own, self.first, 2)

        def across(self, k):
            own = self.block(self.s, k)
            self.send(3 + k, own, self.second, 1)
            self.send(3 + k, own, self.second, -1)

        def along(self):
            low, high = self.block(self.s, 1), self.block(self.s, 2)
            self.landed(0, low)
            if not self.direct:
                self.send(2, self.part(low, 0), self.first, 1)
            self.landed(1, high)
            if not self.direct:
                self.send(2, self.part(high, 1), self.first, -1)

        def turn(self):
            self.landed(2, self.block(self.s, 3))
            if self.direct:
                self.send(7, self.block(self.s, 3), self.second, 2)
            self.across(3)

        def relay(self, k):
            low, high = self.block(shifted(self.s, -1), k), self.block(shifted(self.s, 1), k)
            self.landed(3 + k, self.blocks.at[0:2])
            if self.direct and k == 3:
                return
            self.send(7, self.part(low, 0), self.second, 1)
            self.send(7, self.part(high, 1), self.second, -1)

        def complete(self):
            self.landed(7, self.blocks.at[0:RING])

    row_i = lax.broadcasted_iota(jnp.int32, (WINDOW, 3 * WINDOW), 0)
    col_j = lax.broadcasted_iota(jnp.int32, (WINDOW, 3 * WINDOW), 1)
    close = (col_j >= row_i) & (col_j <= row_i + 2 * WINDOW)
    def part_scores(n, r, low, high):
        position = me * length + (n - 1) * WINDOW + col_j
        valid = close & (position >= 0) & (position < length * count)
        query = q_ref[n * WINDOW : (n + 1) * WINDOW, r * HEAD : (r + 1) * HEAD]
        keys = k_ext[:, n * WINDOW + low : n * WINDOW + high]
        scores = jnp.dot(query, keys, preferred_element_type=F32) * HEAD ** (-0.5)
        return jnp.where(valid[:, low:high], scores, NEGATIVE)

    heads_here = [(n, r) for n in range(groups) for r in range(HEADS // KV_HEADS)]
    own_range = [(WINDOW, 3 * WINDOW), (0, 2 * WINDOW)]
    far_range = [(0, WINDOW), (2 * WINDOW, 3 * WINDOW)]
    own_scores = {(n, r): part_scores(n, r, *own_range[n]) for n, r in heads_here}
    halo.wait_recv()
    for n in range(groups):
        band = slice(n * WINDOW, (n + 3) * WINDOW)
        for r in range(HEADS // KV_HEADS):
            far = part_scores(n, r, *far_range[n])
            masked = jnp.concatenate([far, own_scores[n, r]] if n == 0 else [own_scores[n, r], far], axis=1)
            sink = jnp.full((WINDOW, 1), sink_ref[r], F32)
            top = jnp.maximum(jnp.max(masked, axis=-1, keepdims=True), sink)
            probs = jnp.exp(masked - top)
            denom = jnp.sum(probs, axis=-1, keepdims=True) + jnp.exp(sink - top)
            weights = (probs / denom).astype(BF16)
            output = contract_last(weights, v_ext[:, band]).reshape(WINDOW // tokens, tokens, HEAD)
            half = WINDOW // 2
            for c in colors:
                attended[c, spot[orders[c][0]], n * half : (n + 1) * half, r * HEAD : (r + 1) * HEAD] = (
                    output[:, c * part : (c + 1) * part].reshape(half, HEAD).astype(BF16)
                )

    for c in colors:
        first = orders[c][0]
        own = attended.at[c, spot[first]]
        for delta in (2, 1, -1):
            remote(own, own, a_send.at[c], a_recv.at[c], near(first, delta)).start()
    fetched = w_all.at[0, 0 : RING - 1]
    remote(fetched, fetched, w_send.at[0], w_recv.at[0], (me, tp)).wait_recv()
    for c in colors:
        half_blocks = w_all.at[c, :, mine]
        remote(half_blocks, half_blocks, w_send.at[1], w_recv.at[1], (me + 1 - 2 * core, tp)).start()

    for copy in loads[5:9]:
        copy.wait()
    t_row = lax.broadcasted_iota(jnp.int32, (tokens, tokens), 0)
    t_col = lax.broadcasted_iota(jnp.int32, (tokens, tokens), 1)

    def as_column(row):
        spread = jnp.where(t_row == t_col, jnp.broadcast_to(row, (tokens, tokens)), 0.0)
        return jnp.sum(spread, axis=1, keepdims=True)

    named = [routes_ref[a : a + 1, :].astype(F32) for a in range(2)]
    named_column = [as_column(row) for row in named]
    slot = []
    for row in named:
        rank = jnp.zeros((1, tokens), F32)
        for column in named_column:
            same = (column == row) & (t_row < t_col)
            rank = rank + jnp.sum(jnp.where(same, 1.0, 0.0), axis=0, keepdims=True)
        slot.append(2.0 * row + rank)
    slot_down = lax.broadcasted_iota(jnp.int32, (2 * count, tokens), 0).astype(F32)
    slot_across = lax.broadcasted_iota(jnp.int32, (tokens, 2 * count), 1).astype(F32)
    placed = jnp.where((slot_down == slot[0]) | (slot_down == slot[1]), 1.0, 0.0).astype(BF16)
    picks = [jnp.where(slot_across == as_column(row), 1.0, 0.0).astype(BF16) for row in slot]
    route_weight = [as_column(rw_ref[a : a + 1, :]) for a in range(2)]

    def both(items, *stages):
        for name, *given in stages:
            for item in items:
                getattr(item, name)(*given)

    handed = w_all.at[0]
    remote(handed, handed, w_send.at[1], w_recv.at[1], (me, tp)).wait_recv()
    for c in colors:
        arriving = attended.at[c, 0 : RING - 1]
        remote(arriving, arriving, a_send.at[c], a_recv.at[c], (me, tp)).wait_recv()
        heads = jnp.concatenate([attended[c, i] for i in range(RING)], axis=1)
        for j in range(RING):
            block = w_all[c, j].reshape(RING * WINDOW, WINDOW)
            share = jnp.dot(heads, block, preferred_element_type=F32)
            for t in range(peers):
                s, f = (t // RING, t % RING) if c == 0 else (t % RING, t // RING)
                shares[c, s, f * part : (f + 1) * part, j * WINDOW : (j + 1) * WINDOW] = share[
                    t * part : (t + 1) * part
                ].astype(BF16)
        second = orders[c][1]
        for delta, place in ((2, 2), (1, 0), (-1, 1)):
            remote(
                shares.at[c, shifted(spot[second], delta)], joined.at[c, place], s_send.at[c], s_recv.at[c],
                near(second, delta),
            ).start()
    for c in colors:
        first, second = orders[c]
        f = spot[first]
        remote(joined.at[c], joined.at[c], s_send.at[c], s_recv.at[c], (me, tp)).wait_recv()
        total = shares[c, spot[second]].astype(F32)
        for i in range(RING - 1):
            total = total + joined[c, i].astype(F32)
        rows_out[c] = total.reshape(RING, part, RING * WINDOW).astype(BF16)
        for delta in (2, 1, -1):
            remote(
                rows_out.at[c, shifted(f, delta)], proj.at[c, f], o_send.at[c], o_recv.at[c], near(first, delta)
            ).start()
        proj[c, f] = rows_out[c, f]
    for c in colors:
        arriving = proj.at[c, 0 : RING - 1]
        remote(arriving, arriving, o_send.at[c], o_recv.at[c], (me, tp)).wait_recv()
    projected = []
    for t in range(peers):
        y, x = t // RING, t % RING
        ends = [proj[0, x, :, y * WINDOW : (y + 1) * WINDOW], proj[1, y, :, x * WINDOW : (x + 1) * WINDOW]]
        projected.append(jnp.concatenate([piece.astype(F32) for piece in ends], axis=0))
    hidden_state = res_ref[...].astype(F32) + jnp.concatenate(projected, axis=1)
    inverse = lax.rsqrt(jnp.mean(hidden_state * hidden_state, axis=-1, keepdims=True) + EPS)
    normed = (hidden_state * inverse * gain_ref[...]).astype(BF16)
    slots = jnp.dot(placed, normed, preferred_element_type=F32).astype(BF16)
    for expert in range(count):
        sending[expert] = slots[2 * expert : 2 * expert + 2, :]

    def dispatch(step):
        to = lax.rem(me + step, count)
        remote(
            sending.at[to], arrived.at[count - step], d_send.at[0], d_recv.at[(count - step) // per], (to, tp)
        ).start()

    pairs = [(u, UNITS - 1 - u) for u in range(UNITS // 2)]
    pairs = [pairs[0], *pairs[2:], pairs[1]]

    def dispatch_pair(step, carry):
        dispatch(step + 1)
        dispatch(count - step)
        return carry

    for low, _ in pairs:
        if low == 0:
            dispatch(1)
        lax.fori_loop(max(low * per, 1), (low + 1) * per, dispatch_pair, 0)
    arrived[0] = sending[me]

    class Reduction:
        def __init__(self, unit, axes, direct):
            self.direct = direct
            self.first, self.second = axes
            self.f, self.s = spot[self.first], spot[self.second]
            self.parts, self.hs, self.fs = p_all.at[unit], half_s.at[unit], full_s.at[unit]
            self.total, self.hf, self.ff = sums.at[unit], half_f.at[unit], full_f.at[unit]
            self.recv_sem = r_recv.at[unit]

        def send(self, number, src, dst, axis, delta):
            remote(src, dst, r_send.at[0], self.recv_sem.at[number], near(axis, delta)).start()

        def landed(self, number, ref):
            remote(ref, ref, r_send.at[0], self.recv_sem.at[number], near("x", 1)).wait_recv()

        def at(self, k):
            return shifted(self.f, (0, -1, 1, 2)[k])

        def begin(self):
            h, far = width // 2, shifted(self.s, 2)
            for k in (3, 1, 2, 0):
                src = self.parts.at[far, self.at(k)]
                self.send(k, src.at[:, 0:h], self.hs.at[k, 0], self.second, 1)
                self.send(k, src.at[:, h:width], self.hs.at[k, 1], self.second, -1)

        def relay(self, k):
            h, fk = width // 2, self.at(k)
            up, down = shifted(self.s, 1), shifted(self.s, -1)
            self.landed(k, self.hs.at[k])
            self.parts[up, fk, :, 0:h] = (
                self.parts[up, fk, :, 0:h].astype(F32) + self.hs[k, 0].astype(F32)
            ).astype(BF16)
            self.send(4 + k, self.parts.at[up, fk], self.fs.at[k, 0], self.second, 1)
            self.parts[down, fk, :, h:width] = (
                self.parts[down, fk, :, h:width].astype(F32) + self.hs[k, 1].astype(F32)
            ).astype(BF16)
            self.send(4 + k, self.parts.at[down, fk], self.fs.at[k, 1], self.second, -1)

        def summed(self, k):
            self.landed(4 + k, self.fs.at[k])
            return self.parts[self.s, self.at(k)].astype(F32) + self.fs[k, 0].astype(F32) + self.fs[k, 1].astype(F32)

        def turn(self):
            h = width // 2
            self.total[3] = self.summed(3).astype(BF16)
            if self.direct:
                self.send(10, self.total.at[3], self.ff.at[2], self.first, 2)
                return
            self.send(8, self.total.at[3, :, 0:h], self.hf.at[0], self.first, 1)
            self.send(9, self.total.at[3, :, h:width], self.hf.at[1], self.first, -1)

        def cross(self, k):
            h, i = width // 2, 2 - k
            block = self.summed(k)
            halves = [block[:, 0:h], block[:, h:width]]
            if not self.direct:
                self.landed(8 + i, self.hf.at[i])
                halves[i] = halves[i] + self.hf[i].astype(F32)
            self.total[k, :, 0:h] = halves[0].astype(BF16)
            self.total[k, :, h:width] = halves[1].astype(BF16)
            self.send(10, self.total.at[k], self.ff.at[i], self.first, 1 - 2 * i)

        def finish(self):
            own = self.summed(0)
            senders = 3 if self.direct else 2
            self.landed(10, self.ff.at[0:senders])
            for i in range(senders):
                own = own + self.ff[i].astype(F32)
            return own

    axes = [orders[2 * u // UNITS] for u in range(UNITS)]
    straight = (pairs[0], pairs[0] + pairs[3])
    gathers = [Gather(x_all, u * peers, axes[u], u in straight[0], g_send.at[0], g_recv.at[u]) for u in range(UNITS)]
    reductions = [Reduction(u, axes[u], u in straight[1]) for u in range(UNITS)]

    def rows_here(u):
        first = 1 if u == 0 else 0
        region = arrived.at[u * per + first : (u + 1) * per]
        remote(region, region, d_send.at[0], d_recv.at[u], (me, tp)).wait_recv()
        place = gathers[u].place(gathers[u].s, 0)
        for j in range(per):
            x_all[place, 2 * j : 2 * j + 2, :] = arrived[u * per + j]

    held = {}

    def mlp_up(pair):
        for u in pair:
            gathers[u].complete()
        flat = jnp.concatenate(
            [x_all[u * peers : (u + 1) * peers].reshape(peers * rows, width) for u in pair], axis=0
        )
        gate = contract_last(flat, wg[...])
        upward = contract_last(flat, wu[...])
        held[pair] = (gate / (1.0 + jnp.exp(-gate)) * upward).astype(BF16)

    def mlp_down(pair):
        step = min(512, width)
        for n in range(0, width, step):
            part = jnp.dot(held[pair], wd[:, n : n + step], preferred_element_type=F32)
            for i, u in enumerate(pair):
                block = part[i * peers * rows : (i + 1) * peers * rows].reshape(RING, RING, rows, step)
                p_all[u, :, :, :, n : n + step] = block.astype(BF16)

    def give_back(u):
        total = reductions[u].finish().astype(BF16)
        for j in range(per):
            o = u * per + j
            if o:
                back_send[o] = total[2 * j : 2 * j + 2, :]
            else:
                back[me] = total[0:2, :]
        for j in range(per):
            o = u * per + j
            if o:
                remote(
                    back_send.at[o], back.at[me], b_send.at[0], b_recv.at[0], (lax.rem(me + o, count), tp)
                ).start()

    for copy in loads[9:]:
        copy.wait()

    def enter(pair):
        for u in pair:
            rows_here(u)
            gathers[u].begin()
        both([gathers[u] for u in pair], ("across", 0))

    def blocks_across(pair):
        both([gathers[u] for u in pair], ("across", 1), ("across", 2))

    def gather_step(name, *given):
        return lambda pair: both([gathers[u] for u in pair], (name, *given))

    def reduce_step(name, *given):
        return lambda pair: both([reductions[u] for u in pair], (name, *given))

    def leave(pair):
        for u in pair:
            give_back(u)

    steps = [
        enter, gather_step("along"), blocks_across, gather_step("relay", 0), gather_step("turn"), gather_step("relay", 1),
        gather_step("relay", 2), gather_step("relay", 3), mlp_up, mlp_down, reduce_step("begin"), reduce_step("relay", 3),
        reduce_step("relay", 1), reduce_step("relay", 2), reduce_step("relay", 0), reduce_step("turn"),
        reduce_step("cross", 2), reduce_step("cross", 1), leave,
    ]
    for i, step in ORDER:
        steps[step](pairs[i])

    from_others = back.at[0 : count - 1]
    returned = remote(from_others, from_others, b_send.at[0], b_recv.at[0], (me, tp))
    returned.wait_recv()
    table = jnp.concatenate([back[expert] for expert in range(count)], axis=0)
    mixture = route_weight[0] * jnp.dot(picks[0], table, preferred_element_type=F32)
    mixture = mixture + route_weight[1] * jnp.dot(picks[1], table, preferred_element_type=F32)
    out_ref[...] = hidden_state + mixture

    returned.wait_send()
    dispatched = sending.at[0 : count - 1]
    remote(dispatched, dispatched, d_send.at[0], b_recv.at[0], (me, tp)).wait_send()
    halo.wait_send()
    remote(fetched, fetched, w_send.at[0], b_recv.at[0], (me, tp)).wait_send()
    remote(handed, handed, w_send.at[1], b_recv.at[0], (me, tp)).wait_send()
    for c in colors:
        sent = attended.at[c, 0 : RING - 1]
        remote(sent, sent, a_send.at[c], b_recv.at[0], (me, tp)).wait_send()
        remote(joined.at[c], joined.at[c], s_send.at[c], b_recv.at[0], (me, tp)).wait_send()
        sent = proj.at[c, 0 : RING - 1]
        remote(sent, sent, o_send.at[c], b_recv.at[0], (me, tp)).wait_send()
    sent = x_all.at[0 : UNITS * (peers - 1)]
    remote(sent, sent, g_send.at[0], b_recv.at[0], (me, tp)).wait_send()
    remote(sent, sent, r_send.at[0], b_recv.at[0], (me, tp)).wait_send()


def local(
    queries, keys, values, sink_logit, out_weight, residual, norm_gain, routes, route_weights,
    gate_weight, up_weight, down_weight,
):
    count = lax.axis_size("sp")
    tokens, width = residual.shape
    length, kv = keys.shape
    inner = gate_weight.shape[2]
    heads = queries.shape[1]
    rows = 2 * count // UNITS
    peers = RING * RING
    dma = pltpu.SemaphoreType.DMA
    given = (
        queries, keys.T, values.T, sink_logit, out_weight.reshape(RING, RING, WINDOW, WINDOW), residual, norm_gain.reshape(1, width), routes.T,
        route_weights.T, jnp.swapaxes(gate_weight, 1, 2), jnp.swapaxes(up_weight, 1, 2), down_weight,
    )
    held = [pltpu.VMEM(a.shape, a.dtype) for a in given[:9]] + [pltpu.VMEM((inner, width), BF16)] * 3
    held[3] = pltpu.SMEM(sink_logit.shape, F32)
    out = pl.pallas_call(
        functools.partial(kernel, count),
        out_shape=jax.ShapeDtypeStruct((tokens, width), F32),
        in_specs=[pl.BlockSpec(memory_space=pl.ANY)] * len(given),
        out_specs=pl.BlockSpec(memory_space=pltpu.VMEM),
        scratch_shapes=[
            *held,
            pltpu.VMEM((kv, length + 2 * WINDOW), BF16),
            pltpu.VMEM((kv, length + 2 * WINDOW), BF16),
            pltpu.VMEM((2, RING, RING, WINDOW, WINDOW), BF16),
            pltpu.VMEM((2, RING, length // 2, heads), BF16),
            pltpu.VMEM((2, RING, RING * tokens // 2, RING * WINDOW), BF16),
            pltpu.VMEM((2, RING - 1, RING * tokens // 2, RING * WINDOW), BF16),
            pltpu.VMEM((2, RING, tokens // 2, RING * WINDOW), BF16),
            pltpu.VMEM((2, RING, tokens // 2, RING * WINDOW), BF16),
            pltpu.VMEM((count, 2, width), BF16),
            pltpu.VMEM((count, 2, width), BF16),
            pltpu.VMEM((UNITS * peers, rows, width), BF16),
            pltpu.VMEM((UNITS, RING, RING, rows, width), BF16),
            pltpu.VMEM((UNITS, RING, 2, rows, width // 2), BF16),
            pltpu.VMEM((UNITS, RING, 2, rows, width), BF16),
            pltpu.VMEM((UNITS, RING, rows, width), BF16),
            pltpu.VMEM((UNITS, 2, rows, width // 2), BF16),
            pltpu.VMEM((UNITS, 3, rows, width), BF16),
            pltpu.VMEM((count, 2, width), BF16),
            pltpu.VMEM((count, 2, width), BF16),
            dma((len(given),)),
            dma((1,)),
            dma((1,)),
            dma((2,)),
            dma((2,)),
            dma((2,)),
            dma((2,)),
            dma((2,)),
            dma((2,)),
            dma((2,)),
            dma((2,)),
            dma((1,)),
            dma((UNITS,)),
            dma((1,)),
            dma((1,)),
            dma((1,)),
            dma((UNITS, 8)),
            dma((1,)),
            dma((UNITS, 11)),
        ],
        compiler_params=pltpu.CompilerParams(
            collective_id=0, has_side_effects=True, vmem_limit_bytes=60 * 1024 * 1024
        ),
        name="layer",
    )(*given)
    return out.astype(BF16)


def solution(mesh):
    in_specs = (
        P("sp", "tp"),
        P("sp", "tp"),
        P("sp", "tp"),
        P("tp"),
        P(None, "tp"),
        P(("sp", "tp"), None),
        P(),
        P(("sp", "tp"), None),
        P(("sp", "tp"), None),
        P("sp", None, "tp"),
        P("sp", None, "tp"),
        P("sp", "tp", None),
    )
    out_specs = P(("sp", "tp"), None)
    return jax.shard_map(local, mesh=mesh, in_specs=in_specs, out_specs=out_specs, check_vma=False)
```
